32 devices in a mesh: fs: 16 (over z, y, x), tp: 2 (over core).
Axes of the slice: x: 2, y: 2, z: 4, core: 2. Of those that a mesh axis runs over, the one named last changes fastest.
Arguments:
- tokens: bfloat16 [3072, 2048], P('fs'), may hold values from -6 to 6
- route_ids: int32 [3072, 2], P('fs'), may hold values from 0 to 7, all different within a row; in each aligned block of 192 rows (0 to 191, 192 to 383, ...) at most 96 rows name the same one
- route_logits: float32 [3072, 2], P('fs'), may hold values from -6 to 6
- norm_gain: float32 [2048], P('fs'), may hold values from 0.1 to 1.9
- gate_weight: float32 [8, 2048, 2048], P(None, 'fs', 'tp'), may hold values from -0.125 to 0.125
- up_weight: float32 [8, 2048, 2048], P(None, 'fs', 'tp'), may hold values from -0.125 to 0.125
- down_weight: float32 [8, 2048, 2048], P(None, 'fs', 'tp'), may hold values from -0.125 to 0.125
Outputs:
- mixed: bfloat16 [3072, 2048], P('fs')
- gate_copies: bfloat16 [16, 2048, 2048], P('fs', None, 'tp')
- up_copies: bfloat16 [16, 2048, 2048], P('fs', None, 'tp')
- down_copies: bfloat16 [16, 2048, 2048], P('fs', None, 'tp')
The draws below stay inside these ranges and needn't reach their ends.
Inputs may be any that keep to these rules, and one draw needn't show every extreme that they name: `route_ids`: each row names 2 different experts. Among the rows of one index of fs no expert is named by more than 96 rows, a bound that some of them reach.
All inputs are finite; a program needn't handle non-finite values.
Results may differ from the reference program's by a relative error of at most 0.014.
Values may be sent and summed in bfloat16 or wider, within the bound.
A program may use at most 128 MiB of HBM per device.

```python
import math
import jax
import jax.numpy as jnp
import numpy as np
from jax import lax

D = 2048
FF = 2048
EXPERTS = 8
TOP = 2
TOK_DEV = 192
CAP = 96
TOKENS = 3072
N_FS = 16
N_TP = 2


def levels(key, extent, split, low, high):
    def one(dim, blocks):
        steps = jax.random.uniform(jax.random.fold_in(jax.random.fold_in(key, 6), dim), (blocks,), jnp.float32, low / len(split), high / len(split))
        return jnp.repeat(jnp.exp(steps), extent[dim] // blocks).reshape((-1,) + (1,) * (len(extent) - dim - 1))

    level = one(*split[0])
    for cut in split[1:]:
        level = level * one(*cut)
    return level


def deal_out(rng, own, number, rows, number_of, top, most, lean):
    ranking = jax.random.permutation(rng, number_of)
    packed, usual = load_shares(number_of, rows * top, most, lean, True), load_shares(number_of, rows * top, most, lean, False)
    places = jnp.arange(number_of)

    def named(tallies, rotation):
        used = int((tallies > 0).sum())
        fixed = max(1, used // 4)
        moved = fixed + (places - fixed + rotation * (used - fixed)) % max(1, number_of - fixed)
        return jnp.zeros((number_of,), jnp.int32).at[ranking[jnp.where(places < fixed, places, moved)]].set(jnp.asarray(tallies, jnp.int32))

    tallies = jnp.where(number % 4 == 0, named(packed, number // 4), named(usual, number - number // 4 - 1))
    mixed = jax.random.permutation(jax.random.fold_in(own, 3), number_of)
    donor, sink = mixed[0:number_of // 2 * 2:2], mixed[1:number_of // 2 * 2:2]
    margin = jnp.minimum(tallies[donor] - 1, most - tallies[sink]) // 2
    margin = jnp.where((donor == ranking[0]) | (sink == ranking[0]) | (tallies[sink] == 0), 0, jnp.maximum(margin, 0))
    moved = jax.random.randint(jax.random.fold_in(own, 4), (number_of // 2,), 0, 1 << 20) % (margin + 1)
    tallies = tallies.at[donor].add(-moved).at[sink].add(moved)
    labels = jnp.searchsorted(jnp.cumsum(tallies), jnp.arange(rows * top), side="right").astype(jnp.int32)
    grid = labels.reshape(top, rows).T
    grid = grid[jax.random.permutation(jax.random.fold_in(own, 1), rows)]
    rotation = jax.random.randint(jax.random.fold_in(own, 2), (rows, 1), 0, top)
    return jnp.take_along_axis(grid, (jnp.arange(top)[None, :] + rotation) % top, axis=1)


def load_shares(amount, total, reach, skew, full):
    weights = [(1 << 20) // math.isqrt(rank ** skew) + 1 for rank in range(1, amount + 1)]
    largest = reach if full else min(reach, max(-(-total // amount), total * weights[0] // sum(weights)))
    least = 1 if total - largest >= amount - 1 else 0
    given, rest = [largest] + [least] * (amount - 1), total - largest - least * (amount - 1)
    while rest > 0:
        candidates = [i for i in range(1, amount) if given[i] < largest] or [i for i in range(1, amount) if given[i] < reach]
        pool, left = sum([weights[i] for i in candidates]), rest
        for i in candidates:
            more = min(reach - given[i], max(1, left * weights[i] // pool), rest)
            given[i] = given[i] + more
            rest = rest - more
    return np.array(given)


def centred(stream_key, extent, deviation, limit, cuts=(), held_as=jnp.bfloat16):
    result = deviation * jax.random.normal(stream_key, extent, jnp.float32)
    if cuts:
        result = result * levels(stream_key, extent, cuts, -0.22, 0.18)
    return jnp.clip(result, -limit, limit).astype(held_as)


def setup_inputs(seed: int = 0) -> dict:
    seeds = jax.random.split(jax.random.key(seed), 8)
    tokens = centred(seeds[0], (TOKENS, D), 1.0, 6.0, ((0, 16),))
    route_ids_keys = jax.random.split(jax.random.fold_in(seeds[1], 1), TOKENS // TOK_DEV)
    route_ids_turns = jax.random.permutation(jax.random.fold_in(seeds[1], 3), TOKENS // TOK_DEV)
    route_ids = jax.vmap(lambda own, number: deal_out(jax.random.fold_in(seeds[1], 2), own, number, TOK_DEV, EXPERTS, TOP, CAP, 1))(route_ids_keys, route_ids_turns).reshape((TOKENS, TOP))
    route_logits = centred(seeds[2], (TOKENS, TOP), 1.5, 6.0, ((0, 16),), jnp.float32)
    norm_gain = jnp.clip(1.0 + 0.18 * jax.random.normal(seeds[3], (D,), jnp.float32), 0.1, 1.9)
    gate_weight = centred(seeds[4], (EXPERTS, D, FF), D ** -0.5, 0.125, ((1, 16), (2, 2)), jnp.float32)
    up_weight = centred(seeds[5], (EXPERTS, D, FF), D ** -0.5, 0.125, ((1, 16), (2, 2)), jnp.float32)
    down_weight = centred(seeds[6], (EXPERTS, D, FF), FF ** -0.5, 0.125, ((1, 16), (2, 2)), jnp.float32)
    return dict(tokens=tokens, route_ids=route_ids, route_logits=route_logits, norm_gain=norm_gain, gate_weight=gate_weight, up_weight=up_weight, down_weight=down_weight)


def expert_rows(rows, gate_matrix, up_matrix, down_matrix):
    gate_act = jnp.dot(rows, gate_matrix, preferred_element_type=jnp.float32)
    up_act = jnp.dot(rows, up_matrix, preferred_element_type=jnp.float32)
    hidden = (jax.nn.silu(gate_act) * up_act).astype(jnp.bfloat16)
    row_count = rows.shape[0]
    blocks = hidden.reshape(row_count, N_TP, FF // N_TP).astype(jnp.float32)
    down_blocks = down_matrix.reshape(D, N_TP, FF // N_TP).astype(jnp.float32)
    partial_value = jnp.einsum('rbf,dbf->brd', blocks, down_blocks)
    rounded = lax.optimization_barrier(partial_value.astype(jnp.bfloat16))
    return lax.optimization_barrier(jnp.sum(rounded.astype(jnp.float32), axis=0)).astype(jnp.bfloat16)

def reference(tokens, route_ids, route_logits, norm_gain, gate_weight, up_weight, down_weight):
    copies = N_FS // EXPERTS
    folded_gate = (norm_gain[None, :, None] * gate_weight).astype(jnp.bfloat16)
    folded_up = (norm_gain[None, :, None] * up_weight).astype(jnp.bfloat16)
    down_cast = down_weight.astype(jnp.bfloat16)
    gate_copies = jnp.repeat(folded_gate, copies, axis=0)
    up_copies = jnp.repeat(folded_up, copies, axis=0)
    down_copies = jnp.repeat(down_cast, copies, axis=0)
    values = tokens.astype(jnp.float32)
    center = lax.optimization_barrier(jnp.mean(values, axis=1, keepdims=True))
    spread = lax.optimization_barrier(jnp.mean(jnp.square(values - center), axis=1, keepdims=True))
    normed = ((values - center) * lax.rsqrt(spread + 1e-06)).astype(jnp.bfloat16)
    per_source = route_ids.reshape(N_FS, TOK_DEV * TOP)
    onehot_table = (per_source[:, :, None] == jnp.arange(EXPERTS, dtype=jnp.int32)[None, None, :]).astype(jnp.int32)
    before = jnp.cumsum(onehot_table, axis=1) - onehot_table
    order_rank = lax.optimization_barrier(jnp.sum(before * onehot_table, axis=2))
    source = jnp.arange(N_FS, dtype=jnp.int32)[:, None]
    position = source * CAP + order_rank
    owners = source * TOK_DEV + jnp.arange(TOK_DEV * TOP, dtype=jnp.int32)[None, :] // TOP
    slot_token = jnp.full((EXPERTS, N_FS * CAP), TOKENS, jnp.int32).at[per_source, position].set(owners)
    padded = jnp.concatenate([normed, jnp.zeros((1, D), jnp.bfloat16)], axis=0)

    def one_expert(index):
        rows = padded[slot_token[index]]
        return expert_rows(rows, folded_gate[index], folded_up[index], down_cast[index])
    results = lax.map(one_expert, jnp.arange(EXPERTS, dtype=jnp.int32))
    picked = results[per_source, position].reshape(TOKENS, TOP, D).astype(jnp.float32)
    first_weight = jax.nn.sigmoid(route_logits[:, 0] - route_logits[:, 1])
    second_weight = jax.nn.sigmoid(route_logits[:, 1] - route_logits[:, 0])
    mixed = (first_weight[:, None] * picked[:, 0] + second_weight[:, None] * picked[:, 1]).astype(jnp.bfloat16)
    return (mixed, gate_copies, up_copies, down_copies)
```

```python
import functools
import math

import jax
import jax.numpy as jnp
from jax import lax
from jax.experimental import pallas as pl
from jax.experimental.pallas import tpu as pltpu
from jax.sharding import PartitionSpec as P

MESH = pl.DeviceIdType.MESH
BF16 = jnp.bfloat16
F32 = jnp.float32


def layer(
    experts,
    copies,
    tps,
    tokens,
    ids,
    logits,
    gain,
    gate_in,
    up_in,
    down_in,
    mixed_out,
    gate_out,
    up_out,
    down_out,
    tok,
    gain_col,
    stage,
    send,
    full,
    rows_in,
    table,
    scale,
    hidden,
    part,
    part_in,
    share,
    arrived,
    mixed,
    load_sem,
    w_send,
    w_recv,
    r_send,
    r_recv,
    t_send,
    t_recv,
    s_send,
    s_recv,
    tx_send,
    tx_recv,
    p_send,
    p_recv,
    g_send,
    g_recv,
    f_send,
    f_recv,
    out_sem,
    tok_sem,
):
    shard, cols = stage.shape[2], stage.shape[3]
    tok_rows, width = tok.shape
    block = width // tps
    chunk_f = min(256, cols)
    chunk_w = width // experts
    n_f, n_w = cols // chunk_f, experts // tps
    bits = experts.bit_length() - 1
    half = experts // 2
    me = lax.axis_index("fs")
    tp = lax.axis_index("tp")
    group = lax.div(me, copies)
    lane = lax.rem(me, copies)
    weights = (gate_in, up_in, down_in)
    outs = (gate_out, up_out, down_out)

    place = sum(
        lax.rem(lax.div(group, 1 << i), 2) * (1 << (bits - 1 - i)) for i in range(bits)
    )

    def ahead(d):
        return lax.bitwise_xor(group, jnp.int32(d))

    def twin(c):
        return lax.rem(lane + c, copies)

    def mate(p):
        return lax.rem(tp + p, tps)

    def kept(k):
        return lax.div(place, 1 << k) * (1 << k)

    def other(k):
        return lax.bitwise_xor(kept(k), jnp.int32(1 << k))

    def hop(k):
        return ahead(experts >> (k + 1)) * copies + lane

    def rows(b, k=0):
        return pl.ds(pl.multiple_of(b * tok_rows, 16), tok_rows << k)

    def own_cols(q):
        return pl.ds(pl.multiple_of(q * block, 128), block)

    def features(e):
        return pl.ds(pl.multiple_of(e * chunk_w, 128), chunk_w)

    def shard_rows(g, c):
        return pl.ds(pl.multiple_of((g * copies + c) * shard, 32), shard)

    def loop(lo, hi, body):
        def step(i, carry):
            body(i)
            return carry

        lax.fori_loop(lo, hi, step, 0)

    def remote(src, dst, s_sem, r_sem, fs_to, tp_to):
        return pltpu.make_async_remote_copy(
            src_ref=src,
            dst_ref=dst,
            send_sem=s_sem,
            recv_sem=r_sem,
            device_id=(fs_to, tp_to),
            device_id_type=MESH,
        )

    def load(m, h):
        return pltpu.make_async_copy(weights[m].at[h], stage.at[m, h], load_sem.at[m, h])

    def direct(m, h, s):
        return remote(
            send.at[m, h],
            full.at[m, shard_rows(s, lane)],
            w_send.at[m, h],
            w_recv.at[m, s],
            h * copies + lane,
            tp,
        )

    def relay(m, s, c, to):
        return remote(
            full.at[m, shard_rows(s, c)],
            full.at[m, shard_rows(s, c)],
            r_send.at[m, s, to],
            r_recv.at[m, s, c],
            group * copies + to,
            tp,
        )

    def gather(k, b):
        span = rows_in.at[rows(b, k), own_cols(tp)]
        return remote(span, span, t_send.at[k], t_recv.at[k], hop(k), tp)

    def share_table(k, b):
        span = table.at[pl.ds(b, 1 << k)]
        return remote(span, span, s_send.at[k], s_recv.at[k], hop(k), tp)

    def spread(k, q, p):
        span = rows_in.at[rows(other(k), k), own_cols(q)]
        return remote(span, span, tx_send.at[k, p], tx_recv.at[k, p], me, mate(p))

    def partial(e):
        owner, j = lax.rem(e, tps), lax.div(e, tps)
        p = lax.rem(owner - tp + tps, tps)
        return remote(
            part.at[:, features(e)],
            part_in.at[p - 1, :, features(j)],
            p_send.at[e],
            p_recv.at[p - 1, j],
            me,
            owner,
        )

    def partial_in(p, j):
        span = part_in.at[p - 1, :, features(j)]
        return remote(span, span, p_send.at[0], p_recv.at[p - 1, j], me, mate(p))

    def landing(k):
        return pl.ds(((1 << k) - 1) * tok_rows, tok_rows << k)

    def reduce(k, j):
        return remote(
            share.at[rows(other(k), k), features(j)],
            arrived.at[landing(k), features(j)],
            g_send.at[k, j],
            g_recv.at[k, j],
            hop(k),
            tp,
        )

    def fan(q, j, p):
        span = mixed.at[:, features(j * tps + q)]
        return remote(span, span, f_send.at[j, p], f_recv.at[j, p], me, mate(p))

    tok_copy = pltpu.make_async_copy(tokens, tok, tok_sem)
    tok_copy.start()
    for m in range(3):
        loop(0, experts, lambda d, m=m: load(m, ahead(d)).start())

    barrier = pltpu.get_barrier_semaphore()
    for d in range(1, experts):
        pl.semaphore_signal(
            barrier, inc=1, device_id=(ahead(d) * copies + lane, tp), device_id_type=MESH
        )
    for c in range(1, copies):
        pl.semaphore_signal(
            barrier, inc=1, device_id=(group * copies + twin(c), tp), device_id_type=MESH
        )
    for p in range(1, tps):
        pl.semaphore_signal(barrier, inc=1, device_id=(me, mate(p)), device_id_type=MESH)

    down_rows = lax.broadcasted_iota(jnp.int32, (shard, shard), 0)
    across = lax.broadcasted_iota(jnp.int32, (shard, shard), 1)
    gain_col[...] = jnp.sum(
        jnp.where(down_rows == across, gain[...], 0.0), axis=1, keepdims=True
    )

    gap = logits[0:1, :] - logits[1:2, :]
    choice = (1.0 / (1.0 + jnp.exp(-gap)), 1.0 / (1.0 + jnp.exp(gap)))
    named = lax.broadcasted_iota(jnp.int32, (experts, tok_rows), 0)
    table[place] = jnp.zeros(table.shape[1:], F32)
    table[place, :, 0:tok_rows] = sum(
        jnp.where(ids[k : k + 1, :] == named, choice[k], 0.0) for k in range(2)
    )

    tok_copy.wait()
    step_rows = math.gcd(tok_rows, 32)

    def normalize(i):
        at = pl.multiple_of(i * step_rows, 16)
        values = tok[pl.ds(at, step_rows), :].astype(F32)
        values = values - jnp.mean(values, axis=1, keepdims=True)
        var = jnp.mean(values * values, axis=1, keepdims=True)
        where = pl.ds(pl.multiple_of(place * tok_rows + at, 16), step_rows)
        rows_in[where, :] = (values * lax.rsqrt(var + 1e-06)).astype(BF16)

    loop(0, tok_rows // step_rows, normalize)

    def rounded(m, h):
        load(m, h).wait()
        value = stage[m, h]
        if m < 2:
            value = gain_col[...] * value
        return value.astype(BF16)

    full[0, shard_rows(group, lane)] = rounded(0, group)

    pl.semaphore_wait(barrier, experts + copies + tps - 3)

    gather(0, kept(0)).start()
    share_table(0, kept(0)).start()

    def convert(m, lo, hi):
        def one(d):
            send[m, ahead(d)] = rounded(m, ahead(d))

        loop(lo, hi, one)

    def start(m, lo, hi):
        loop(lo, hi, lambda d: direct(m, ahead(d), group).start())

    def relay_own(m):
        for c in range(1, copies):
            relay(m, group, lane, twin(c)).start()

    early = half + max(half // 2, 1)
    convert(0, half, early)
    relay_own(0)
    start(0, half, early)
    convert(0, 1, 2)
    for m in range(1, 3):
        full[m, shard_rows(group, lane)] = rounded(m, group)
        start(m - 1, 1, 2)
        convert(m, 1, 2)
        relay_own(m)
    start(2, 1, 2)
    convert(0, early, experts)
    convert(0, 2, half)
    convert(1, half, experts)
    convert(1, 2, half)
    convert(2, half, experts)
    convert(2, 2, half)

    def relay_step(m, d):
        s = ahead(d)
        direct(m, s, s).wait_recv()
        for c in range(1, copies):
            relay(m, s, lane, twin(c)).start()

    def relay_wait(m, s):
        for c in range(1, copies):
            relay(m, s, twin(c), lane).wait_recv()

    def gathered(k):
        gather(k, other(k)).wait_recv()
        share_table(k, other(k)).wait_recv()
        if k + 1 < bits:
            gather(k + 1, kept(k + 1)).start()
            share_table(k + 1, kept(k + 1)).start()
        for p in range(1, tps):
            spread(k, tp, p).start()

    def relays(m, lo, hi):
        loop(lo, hi, lambda d: relay_step(m, d))

    for m in range(3):
        relays(m, 1, 2)
    gathered(0)
    start(0, early, experts)
    start(0, 2, half)
    start(1, half, early)
    relays(0, half, early)
    for k in range(1, bits - 1):
        gathered(k)
    start(1, early, experts)
    start(1, 2, half)
    relays(0, 2, half)
    relays(0, early, experts)
    start(2, half, experts)
    start(2, 2, half)
    relays(1, half, early)
    relays(1, 2, half)
    gathered(bits - 1)
    relays(1, early, experts)

    def set_scale(b):
        row = table[b, pl.ds(group, 1), :]
        column = jnp.transpose(jnp.broadcast_to(row, (128, row.shape[1])))
        scale[rows(b), :] = column[:tok_rows]

    loop(0, experts, set_scale)

    def out_copy(m):
        return pltpu.make_async_copy(full.at[m], outs[m].at[0], out_sem.at[m])

    for m in range(2):
        loop(0, experts, lambda s, m=m: relay_wait(m, s))
        out_copy(m).start()

    n_pre = min(half - 1, 2 * n_f)
    for part_no in range(2):
        last = bits - 1
        span = rows((kept(last), other(last))[part_no], last)
        for k in range(bits - 1) if part_no == 0 else (bits - 1,):
            for p in range(1, tps):
                spread(k, mate(tps - p), p).wait_recv()

        def gate_up(c):
            if part_no == 0:
                @pl.when(c < min(n_pre, n_f))
                def _():
                    relay_step(2, 2 + c)

            where = pl.ds(pl.multiple_of(c * chunk_f, 128), chunk_f)
            gate = jnp.dot(rows_in[span, :], full[0, :, where], preferred_element_type=F32)
            up = jnp.dot(rows_in[span, :], full[1, :, where], preferred_element_type=F32)
            hidden[span, where] = (gate / (1.0 + jnp.exp(-gate)) * up).astype(BF16)

        loop(0, n_f, gate_up)

    relays(2, 2 + min(n_pre, n_f), half + 1)

    def add_up(e):
        @pl.when(lax.rem(e, tps) == tp)
        def _():
            j = lax.div(e, tps)
            for p in range(1, tps):
                partial_in(p, j).wait_recv()

            def one(b):
                for q in range(chunk_w // 128):
                    here = pl.ds(pl.multiple_of(e * chunk_w + q * 128, 128), 128)
                    there = pl.ds(pl.multiple_of(j * chunk_w + q * 128, 128), 128)
                    total = part[rows(b), here].astype(F32)
                    for p in range(1, tps):
                        total = total + part_in[p - 1, rows(b), there].astype(F32)
                    share[rows(b), there] = (scale[rows(b), :] * total).astype(BF16)

            first = other(bits - 1)
            loop(first, first + half, one)
            reduce(bits - 1, j).start()
            first = kept(bits - 1)
            loop(first, first + half, one)

    def down_step(d):
        e = ahead(d)
        relay_wait(2, e)
        part[:, features(e)] = lax.dot_general(
            hidden[...],
            full[2, features(e), :],
            (((1,), (1,)), ((), ())),
            preferred_element_type=F32,
        ).astype(BF16)

        @pl.when(lax.rem(e, tps) != tp)
        def _():
            partial(e).start()

    def owned(i):
        e = ahead(tps * i + lax.bitwise_xor(tp, lax.rem(group, tps)))
        return lax.div(e, tps)

    def reduce_step(k, i):
        j = owned(i)
        reduce(k, j).wait_recv()

        def one(b):
            here = rows(kept(k) + b)
            come = pl.ds(pl.multiple_of(((1 << k) - 1 + b) * tok_rows, 16), tok_rows)
            total = share[here, features(j)].astype(F32) + arrived[come, features(j)].astype(F32)
            if k > 0:
                share[here, features(j)] = total.astype(BF16)
            else:
                mixed[:, features(j * tps + tp)] = total.astype(BF16)

        loop(0, 1 << k, one)
        if k > 0:
            reduce(k - 1, j).start()
        else:
            for p in range(1, tps):
                fan(tp, j, p).start()

    def near_step(d):
        down_step(d)

        @pl.when(d > 0)
        def _():
            add_up(ahead(d - 1))

    loop(0, half, near_step)
    relays(2, half + 1, early)
    add_up(ahead(half - 1))
    for k in range(bits - 1, 0, -1):
        loop(0, n_w // 2, lambda i, k=k: reduce_step(k, i))

    def far_step(d):
        down_step(d)

        @pl.when(d > half)
        def _():
            add_up(ahead(d - 1))

        @pl.when(d + early - half < experts)
        def _():
            relay_step(2, d + early - half)

    loop(half, experts, far_step)
    out_copy(2).start()
    add_up(ahead(experts - 1))
    for k in range(bits - 1, 0, -1):
        loop(n_w // 2, n_w, lambda i, k=k: reduce_step(k, i))
    loop(n_w // 2, n_w, lambda i: reduce_step(0, i))
    loop(0, n_w // 2, lambda i: reduce_step(0, i))

    def fan_wait(j):
        for p in range(1, tps):
            fan(mate(tps - p), j, p).wait_recv()

    loop(0, n_w, fan_wait)
    last_copy = pltpu.make_async_copy(mixed, mixed_out, tok_sem)
    last_copy.start()

    for k in range(bits):
        gather(k, kept(k)).wait_send()
        share_table(k, kept(k)).wait_send()
        for p in range(1, tps):
            spread(k, tp, p).wait_send()
        loop(0, n_w, lambda j, k=k: reduce(k, j).wait_send())
    for m in range(3):
        loop(1, experts, lambda d, m=m: direct(m, ahead(d), group).wait_send())

        def relays_sent(s, m=m):
            for c in range(1, copies):
                relay(m, s, lane, twin(c)).wait_send()

        loop(0, experts, relays_sent)
        out_copy(m).wait()

    def part_sent(e):
        @pl.when(lax.rem(e, tps) != tp)
        def _():
            partial(e).wait_send()

    loop(0, experts, part_sent)

    def fans_sent(j):
        for p in range(1, tps):
            fan(tp, j, p).wait_send()

    loop(0, n_w, fans_sent)
    last_copy.wait()


def body(tokens, route_ids, route_logits, norm_gain, gate_weight, up_weight, down_weight):
    experts, shard, cols = gate_weight.shape
    fs_count, tps = lax.axis_size("fs"), lax.axis_size("tp")
    copies = fs_count // experts
    tok_rows, width = tokens.shape
    block = width // tps
    n_rows = experts * tok_rows
    depth = shard * fs_count
    n_w = experts // tps
    bits = experts.bit_length() - 1
    assert experts == 1 << bits and bits > 1
    assert tps & (tps - 1) == 0 and n_w * tps == experts

    dma = pltpu.SemaphoreType.DMA
    anywhere = pl.BlockSpec(memory_space=pl.ANY)
    inside = pl.BlockSpec(memory_space=pltpu.VMEM)
    copy_shape = jax.ShapeDtypeStruct((1, depth, cols), BF16)
    return pl.pallas_call(
        functools.partial(layer, experts, copies, tps),
        out_shape=(jax.ShapeDtypeStruct((tok_rows, width), BF16),) + (copy_shape,) * 3,
        in_specs=[anywhere] + [inside] * 3 + [anywhere] * 3,
        out_specs=(anywhere,) * 4,
        scratch_shapes=[
            pltpu.VMEM((tok_rows, width), BF16),
            pltpu.VMEM((shard, 1), F32),
            pltpu.VMEM((3, experts, shard, cols), F32),
            pltpu.VMEM((3, experts, shard, cols), BF16),
            pltpu.VMEM((3, depth, cols), BF16),
            pltpu.VMEM((n_rows, width), BF16),
            pltpu.VMEM((experts, experts, -(-tok_rows // 128) * 128), F32),
            pltpu.VMEM((n_rows, 128), F32),
            pltpu.VMEM((n_rows, cols), BF16),
            pltpu.VMEM((n_rows, width), BF16),
            pltpu.VMEM((tps - 1, n_rows, block), BF16),
            pltpu.VMEM((n_rows, block), BF16),
            pltpu.VMEM((n_rows - tok_rows, block), BF16),
            pltpu.VMEM((tok_rows, width), BF16),
            dma((3, experts)),
            dma((3, experts)),
            dma((3, experts)),
            dma((3, experts, copies)),
            dma((3, experts, copies)),
            dma((bits,)),
            dma((bits,)),
            dma((bits,)),
            dma((bits,)),
            dma((bits, tps)),
            dma((bits, tps)),
            dma((experts,)),
            dma((tps - 1, n_w)),
            dma((bits, n_w)),
            dma((bits, n_w)),
            dma((n_w, tps)),
            dma((n_w, tps)),
            dma((3,)),
            dma,
        ],
        compiler_params=pltpu.CompilerParams(
            collective_id=0, has_side_effects=True, vmem_limit_bytes=64 * 1024 * 1024 - 65536
        ),
        name="layer",
    )(
        tokens,
        route_ids.T,
        route_logits.T,
        norm_gain[None, :],
        gate_weight,
        up_weight,
        down_weight,
    )


def solution(mesh):
    return jax.shard_map(
        body,
        mesh=mesh,
        in_specs=(
            P("fs", None),
            P("fs", None),
            P("fs", None),
            P("fs"),
            P(None, "fs", "tp"),
            P(None, "fs", "tp"),
            P(None, "fs", "tp"),
        ),
        out_specs=(P("fs", None), P("fs", None, "tp"), P("fs", None, "tp"), P("fs", None, "tp")),
        check_vma=False,
    )
```

```python
import functools
import math

import jax
import jax.numpy as jnp
from jax import lax
from jax.experimental import pallas as pl
from jax.experimental.pallas import tpu as pltpu
from jax.sharding import PartitionSpec as P

CAP = 96
MESH = pl.DeviceIdType.MESH
BF16 = jnp.bfloat16
F32 = jnp.float32


def layer(
    experts,
    copies,
    tps,
    tokens,
    ids,
    logits,
    gain,
    gate_in,
    up_in,
    down_in,
    mixed_out,
    gate_out,
    up_out,
    down_out,
    tok,
    gain_col,
    stage,
    send,
    full,
    rows_in,
    table,
    rank,
    packed,
    unpack,
    scale,
    hidden,
    part,
    part_in,
    outbox,
    pair,
    share,
    arrived,
    mixed,
    load_sem,
    w_send,
    w_recv,
    r_send,
    r_recv,
    t_send,
    t_recv,
    s_send,
    s_recv,
    tx_send,
    tx_recv,
    p_send,
    p_recv,
    g_send,
    g_recv,
    f_send,
    f_recv,
    out_sem,
    tok_sem,
):
    shard, cols = stage.shape[2], stage.shape[3]
    tok_rows, width = tok.shape
    block = width // tps
    chunk_f = min(256, cols)
    chunk_w = width // experts
    n_f, n_w = cols // chunk_f, experts // tps
    bits = experts.bit_length() - 1
    half = experts // 2
    me = lax.axis_index("fs")
    tp = lax.axis_index("tp")
    group = lax.div(me, copies)
    lane = lax.rem(me, copies)
    weights = (gate_in, up_in, down_in)
    outs = (gate_out, up_out, down_out)

    def mirror(o):
        return int(f"{o:0{bits}b}"[::-1], 2)

    place = sum(
        lax.rem(lax.div(group, 1 << i), 2) * (1 << (bits - 1 - i)) for i in range(bits)
    )

    at_end = lax.rem(lax.div(group, half), 2) == lax.rem(lax.div(group, half // 2), 2)

    def turn(d):
        swapped = lax.bitwise_xor(jnp.int32(d), jnp.int32(half // 2))
        return lax.select(jnp.logical_and(at_end, d >= half), swapped, jnp.int32(d))

    def ahead(d):
        return lax.bitwise_xor(group, jnp.int32(d))

    def twin(c):
        return lax.rem(lane + c, copies)

    def mate(p):
        return lax.rem(tp + p, tps)

    def kept(k):
        return lax.div(place, 1 << k) * (1 << k)

    def other(k):
        return lax.bitwise_xor(kept(k), jnp.int32(1 << k))

    def hop(k):
        return ahead(experts >> (k + 1)) * copies + lane

    def rows(b, k=0):
        return pl.ds(pl.multiple_of(b * tok_rows, 16), tok_rows << k)

    def slots(b):
        return pl.ds(pl.multiple_of(b * CAP, 16), CAP)

    def own_cols(q):
        return pl.ds(pl.multiple_of(q * block, 128), block)

    def features(e):
        return pl.ds(pl.multiple_of(e * chunk_w, 128), chunk_w)

    def shard_rows(g, c):
        return pl.ds(pl.multiple_of((g * copies + c) * shard, 32), shard)

    def loop(lo, hi, body):
        def step(i, carry):
            body(i)
            return carry

        lax.fori_loop(lo, hi, step, 0)

    def remote(src, dst, s_sem, r_sem, fs_to, tp_to):
        return pltpu.make_async_remote_copy(
            src_ref=src,
            dst_ref=dst,
            send_sem=s_sem,
            recv_sem=r_sem,
            device_id=(fs_to, tp_to),
            device_id_type=MESH,
        )

    def load(m, h):
        return pltpu.make_async_copy(weights[m].at[h], stage.at[m, h], load_sem.at[m, h])

    def direct(m, h, s):
        return remote(
            send.at[m, h],
            full.at[m, shard_rows(s, lane)],
            w_send.at[m, h],
            w_recv.at[m, s],
            h * copies + lane,
            tp,
        )

    def relay(m, s, c, to):
        return remote(
            full.at[m, shard_rows(s, c)],
            full.at[m, shard_rows(s, c)],
            r_send.at[m, s, to],
            r_recv.at[m, s, c],
            group * copies + to,
            tp,
        )

    def at_offset(o):
        return lax.bitwise_xor(place, jnp.int32(mirror(o)))

    def gather(o, b):
        span = rows_in.at[rows(at_offset(o)), own_cols(tp)]
        return remote(span, span, t_send.at[o ^ b], t_recv.at[o ^ b], ahead(b) * copies + lane, tp)

    def share_table(o, b):
        span = table.at[at_offset(o)]
        return remote(span, span, s_send.at[o ^ b], s_recv.at[o ^ b], ahead(b) * copies + lane, tp)

    def gather_in(o):
        span, row = rows_in.at[rows(at_offset(o)), own_cols(tp)], table.at[at_offset(o)]
        b = ahead(o & -o) * copies + lane
        remote(span, span, t_send.at[o], t_recv.at[o], b, tp).wait_recv()
        remote(row, row, s_send.at[o], s_recv.at[o], b, tp).wait_recv()

    def spread(o, q, p):
        span = rows_in.at[rows(at_offset(o)), own_cols(q)]
        return remote(span, span, tx_send.at[o, p], tx_recv.at[o, p], me, mate(p))

    def partial(e):
        owner, j = lax.rem(e, tps), lax.div(e, tps)
        p = lax.rem(owner - tp + tps, tps)
        return remote(
            part.at[:, features(e)],
            part_in.at[p - 1, :, features(j)],
            p_send.at[e],
            p_recv.at[p - 1, j],
            me,
            owner,
        )

    def partial_in(p, j):
        span = part_in.at[p - 1, :, features(j)]
        return remote(span, span, p_send.at[0], p_recv.at[p - 1, j], me, mate(p))

    def landing(k):
        return pl.ds(((1 << k) - 1) * tok_rows, tok_rows << k)

    def reduce(k, j):
        if k == bits - 1:
            src = outbox.at[:, :, features(j)]
            dst = pair.at[:, pl.ds(CAP, CAP), features(j)]
        else:
            src = share.at[rows(other(k) - kept(bits - 1), k), features(j)]
            dst = arrived.at[landing(k), features(j)]
        return remote(src, dst, g_send.at[k, j], g_recv.at[k, j], hop(k), tp)

    def fan(q, j, p):
        span = mixed.at[:, features(j * tps + q)]
        return remote(span, span, f_send.at[j, p], f_recv.at[j, p], me, mate(p))

    tok_copy = pltpu.make_async_copy(tokens, tok, tok_sem)
    tok_copy.start()
    for m in range(3):
        loop(0, experts, lambda d, m=m: load(m, ahead(d)).start())

    barrier = pltpu.get_barrier_semaphore()
    for d in range(1, experts):
        pl.semaphore_signal(
            barrier, inc=1, device_id=(ahead(d) * copies + lane, tp), device_id_type=MESH
        )
    for c in range(1, copies):
        pl.semaphore_signal(
            barrier, inc=1, device_id=(group * copies + twin(c), tp), device_id_type=MESH
        )
    for p in range(1, tps):
        pl.semaphore_signal(barrier, inc=1, device_id=(me, mate(p)), device_id_type=MESH)

    down_rows = lax.broadcasted_iota(jnp.int32, (shard, shard), 0)
    across = lax.broadcasted_iota(jnp.int32, (shard, shard), 1)
    gain_col[...] = jnp.sum(
        jnp.where(down_rows == across, gain[...], 0.0), axis=1, keepdims=True
    )

    gap = logits[0:1, :] - logits[1:2, :]
    choice = (1.0 / (1.0 + jnp.exp(-gap)), 1.0 / (1.0 + jnp.exp(gap)))
    named = lax.broadcasted_iota(jnp.int32, (experts, tok_rows), 0)
    table[place] = jnp.zeros(table.shape[1:], F32)
    table[place, :, 0:tok_rows] = sum(
        jnp.where(ids[k : k + 1, :] == named, choice[k], 0.0) for k in range(2)
    )

    phase = jax.named_scope
    tok_copy.wait()
    step_rows = math.gcd(tok_rows, 32)

    def normalize(i):
        at = pl.multiple_of(i * step_rows, 16)
        values = tok[pl.ds(at, step_rows), :].astype(F32)
        values = values - jnp.mean(values, axis=1, keepdims=True)
        var = jnp.mean(values * values, axis=1, keepdims=True)
        where = pl.ds(pl.multiple_of(place * tok_rows + at, 16), step_rows)
        rows_in[where, :] = (values * lax.rsqrt(var + 1e-06)).astype(BF16)

    loop(0, tok_rows // step_rows, normalize)

    def rounded(m, h):
        load(m, h).wait()
        value = stage[m, h]
        if m < 2:
            value = gain_col[...] * value
        return value.astype(BF16)

    full[0, shard_rows(group, lane)] = rounded(0, group)

    with phase("barrier"):
        pl.semaphore_wait(barrier, experts + copies + tps - 3)

    masks = [1 << k for k in range(bits - 1, -1, -1)]

    def forward(o):
        for b in masks:
            if o == 0 or b < o & -o:
                gather(o, b).start()
                share_table(o, b).start()

    forward(0)

    def convert(m, lo, hi):
        def one(d):
            send[m, ahead(d)] = rounded(m, ahead(d))

        loop(lo, hi, one)

    def start(m, lo, hi):
        loop(lo, hi, lambda d: direct(m, ahead(d), group).start())

    def relay_own(m):
        for c in range(1, copies):
            relay(m, group, lane, twin(c)).start()

    def relay_step(m, d):
        s = ahead(turn(d) if m < 2 else d)
        direct(m, s, s).wait_recv()
        for c in range(1, copies):
            relay(m, s, lane, twin(c)).start()

    def relay_wait(m, s):
        for c in range(1, copies):
            relay(m, s, twin(c), lane).wait_recv()

    def gathered(o):
        gather_in(o)
        forward(o)
        for p in range(1, tps):
            spread(o, tp, p).start()

    def relays(m, lo, hi):
        loop(lo, hi, lambda d: relay_step(m, d))

    def out_copy(m):
        return pltpu.make_async_copy(full.at[m], outs[m].at[0], out_sem.at[m])

    early = half + max(half // 2, 1)
    with phase("first"):
        convert(0, 2, early)
        relay_own(0)
        start(0, 2, early)
        convert(0, 1, 2)
        for m in range(1, 3):
            full[m, shard_rows(group, lane)] = rounded(m, group)
            start(m - 1, 1, 2)
            convert(m, 1, 2)
            relay_own(m)
        start(2, 1, 2)
        convert(0, early, experts)
        convert(1, 2, experts)
        convert(2, 2, experts)
    with phase("gate_1"):
        relays(0, 1, 2)
    for o in range(2, half, 2):
        with phase("tok_low"):
            gathered(o)
    with phase("tok_half"):
        gathered(half)
    start(0, early, experts)
    start(1, 2, experts)
    with phase("up_down_1"):
        relays(1, 1, 2)
        relays(2, 1, 2)
    with phase("gate_near"):
        relays(0, 2, half)
    for o in range(half + 2, experts, 2):
        with phase("tok_high"):
            gathered(o)
    start(2, 2, half)
    with phase("gate_far"):
        relays(0, half, experts)
    for o in range(1, experts, 2):
        with phase("tok_odd"):
            gathered(o)

    with phase("gate_wait"):
        for o in range(1, experts):
            for p in range(1, tps):
                spread(o, mate(tps - p), p).wait_recv()

    lanes = table.shape[2]
    before = lax.broadcasted_iota(jnp.int32, (lanes, lanes), 0)
    after = lax.broadcasted_iota(jnp.int32, (lanes, lanes), 1)
    earlier = jnp.where(before < after, 1.0, 0.0).astype(BF16)

    def set_rank(b):
        chosen = table[b] > 0.0
        count = jnp.dot(
            jnp.where(chosen, 1.0, 0.0).astype(BF16), earlier, preferred_element_type=F32
        )
        rank[b] = jnp.where(chosen, count, -4.0 * CAP)

    def pack(b):
        slot = lax.broadcasted_iota(jnp.int32, (CAP, lanes), 0).astype(F32)
        hit = jnp.where(rank[b, pl.ds(group, 1), :] == slot, 1.0, 0.0)
        weight = jnp.sum(hit * table[b, pl.ds(group, 1), :], axis=1, keepdims=True)
        scale[slots(b), :] = jnp.broadcast_to(weight, (CAP, 128))
        packed[slots(b), :] = jnp.dot(
            hit[:, :tok_rows].astype(BF16), rows_in[rows(b), :], preferred_element_type=F32
        ).astype(BF16)

    def column(b, e):
        row = rank[b, pl.ds(e, 1), :]
        return jnp.transpose(jnp.broadcast_to(row, (128, lanes)))[:tok_rows, 0:1]

    def set_unpack(i):
        b = kept(bits - 1) + i
        slot = lax.broadcasted_iota(jnp.int32, (tok_rows, 2 * CAP), 1).astype(F32)
        hit = (column(b, group) == slot) | (column(b, ahead(1)) + CAP == slot)
        unpack[i] = jnp.where(hit, 1.0, 0.0).astype(BF16)

    with phase("set_rank"):
        loop(0, experts, set_rank)
    with phase("pack"):
        loop(0, experts, pack)
    with phase("set_unpack"):
        loop(0, half, set_unpack)

    def project(m, pending):
        def one(c):
            for slot, d in pending:
                @pl.when(c == min(slot, n_f - 1))
                def _():
                    with phase("relay_in"):
                        relay_step(m + 1, d)

            where = pl.ds(pl.multiple_of(c * chunk_f, 128), chunk_f)
            out = jnp.dot(packed[...], full[m, :, where], preferred_element_type=F32)
            if m == 0:
                out = out / (1.0 + jnp.exp(-out))
            else:
                out = out * hidden[:, where].astype(F32)
            hidden[:, where] = out.astype(BF16)

        with phase("project"):
            loop(0, n_f, one)

    with phase("gate_wait"):
        loop(0, experts, lambda s: relay_wait(0, s))
        out_copy(0).start()
    project(0, [(i, 2 + i) for i in range(half)])

    @pl.when(jnp.logical_not(at_end))
    def _():
        start(2, half, experts)

    with phase("up_rest"):
        relays(1, 2 + half, experts)

    with phase("up_wait"):
        loop(0, experts, lambda s: relay_wait(1, s))
        out_copy(1).start()

    @pl.when(at_end)
    def _():
        start(2, half, experts)

    project(1, [(2 * i, 2 + i) for i in range(half - 2)])

    def add_up(e):
        @pl.when(lax.rem(e, tps) == tp)
        def _():
            j = lax.div(e, tps)
            for p in range(1, tps):
                partial_in(p, j).wait_recv()

            def fill(target, first):
                def one(i):
                    b = first + i
                    for q in range(chunk_w // 128):
                        here = pl.ds(pl.multiple_of(e * chunk_w + q * 128, 128), 128)
                        there = pl.ds(pl.multiple_of(j * chunk_w + q * 128, 128), 128)
                        total = part[slots(b), here].astype(F32)
                        for p in range(1, tps):
                            total = total + part_in[p - 1, slots(b), there].astype(F32)
                        target[i, 0:CAP, there] = (scale[slots(b), :] * total).astype(BF16)

                loop(0, half, one)

            fill(outbox, other(bits - 1))
            reduce(bits - 1, j).start()
            fill(pair, kept(bits - 1))

    def down_step(d):
        e = ahead(d)
        relay_wait(2, e)
        part[:, features(e)] = lax.dot_general(
            hidden[...],
            full[2, features(e), :],
            (((1,), (1,)), ((), ())),
            preferred_element_type=F32,
        ).astype(BF16)

        @pl.when(lax.rem(e, tps) != tp)
        def _():
            partial(e).start()

    def owned(i, swap=False):
        d = tps * i + lax.bitwise_xor(tp, lax.rem(group, tps))
        return lax.div(ahead(turn(d) if swap else d), tps)

    def reduce_step(k, i):
        j = owned(i, k < bits - 1)
        reduce(k, j).wait_recv()
        base = kept(k) - kept(bits - 1)

        def one(b):
            here = rows(base + b)
            if k == bits - 1:
                total = jnp.dot(unpack[b], pair[b, :, features(j)], preferred_element_type=F32)
            else:
                come = pl.ds(pl.multiple_of(((1 << k) - 1 + b) * tok_rows, 16), tok_rows)
                total = share[here, features(j)].astype(F32)
                total = total + arrived[come, features(j)].astype(F32)
            if k > 0:
                share[here, features(j)] = total.astype(BF16)
            else:
                mixed[:, features(j * tps + tp)] = total.astype(BF16)

        loop(0, 1 << k, one)
        if k > 0:
            reduce(k - 1, j).start()
        else:
            for p in range(1, tps):
                fan(tp, j, p).start()

    def down_steps(lo, hi):
        def one(d):
            down_step(d)

            @pl.when(d > lo)
            def _():
                add_up(ahead(d - 1))

        with phase("down"):
            loop(lo, hi, one)

    down_steps(0, half)
    with phase("relay_early"):
        relays(2, half, early)
    with phase("near_add"):
        add_up(ahead(half - 1))
    down_steps(half, early)
    with phase("early_add"):
        add_up(ahead(early - 1))
    for k in range(bits - 1, 0, -1):
        with phase(f"near_reduce{k}"):
            loop(0, n_w // 2, lambda i, k=k: reduce_step(k, i))
        with phase("relay_late"):
            lo = early + (bits - 1 - k) * (experts - early) // (bits - 1)
            relays(2, lo, early + (bits - k) * (experts - early) // (bits - 1))
    down_steps(early, experts)
    out_copy(2).start()
    with phase("far_add"):
        add_up(ahead(experts - 1))
    for k in range(bits - 1, 0, -1):
        with phase(f"far_reduce{k}"):
            loop(n_w // 2, n_w, lambda i, k=k: reduce_step(k, i))
    with phase("last_far"):
        loop(n_w // 2, n_w, lambda i: reduce_step(0, i))
    with phase("last_near"):
        loop(0, n_w // 2, lambda i: reduce_step(0, i))

    def fan_wait(j):
        for p in range(1, tps):
            fan(mate(tps - p), j, p).wait_recv()

    with phase("fan_wait"):
        loop(0, n_w, fan_wait)
    last_copy = pltpu.make_async_copy(mixed, mixed_out, tok_sem)
    last_copy.start()

    for o in range(experts):
        for b in masks:
            if o == 0 or b < o & -o:
                gather(o, b).wait_send()
                share_table(o, b).wait_send()
        for p in range(1, tps):
            if o:
                spread(o, tp, p).wait_send()
    for k in range(bits):
        loop(0, n_w, lambda j, k=k: reduce(k, j).wait_send())
    for m in range(3):
        loop(1, experts, lambda d, m=m: direct(m, ahead(d), group).wait_send())

        def relays_sent(s, m=m):
            for c in range(1, copies):
                relay(m, s, lane, twin(c)).wait_send()

        loop(0, experts, relays_sent)
        out_copy(m).wait()

    def part_sent(e):
        @pl.when(lax.rem(e, tps) != tp)
        def _():
            partial(e).wait_send()

    loop(0, experts, part_sent)

    def fans_sent(j):
        for p in range(1, tps):
            fan(tp, j, p).wait_send()

    loop(0, n_w, fans_sent)
    last_copy.wait()


def body(tokens, route_ids, route_logits, norm_gain, gate_weight, up_weight, down_weight):
    experts, shard, cols = gate_weight.shape
    fs_count, tps = lax.axis_size("fs"), lax.axis_size("tp")
    copies = fs_count // experts
    tok_rows, width = tokens.shape
    block = width // tps
    n_rows, n_slots = experts * tok_rows, experts * CAP
    lanes, half = -(-tok_rows // 128) * 128, experts // 2
    depth = shard * fs_count
    n_w = experts // tps
    bits = experts.bit_length() - 1
    assert experts == 1 << bits and bits > 1
    assert tps & (tps - 1) == 0 and n_w * tps == experts

    dma = pltpu.SemaphoreType.DMA
    anywhere = pl.BlockSpec(memory_space=pl.ANY)
    inside = pl.BlockSpec(memory_space=pltpu.VMEM)
    copy_shape = jax.ShapeDtypeStruct((1, depth, cols), BF16)
    return pl.pallas_call(
        functools.partial(layer, experts, copies, tps),
        out_shape=(jax.ShapeDtypeStruct((tok_rows, width), BF16),) + (copy_shape,) * 3,
        in_specs=[anywhere] + [inside] * 3 + [anywhere] * 3,
        out_specs=(anywhere,) * 4,
        scratch_shapes=[
            pltpu.VMEM((tok_rows, width), BF16),
            pltpu.VMEM((shard, 1), F32),
            pltpu.VMEM((3, experts, shard, cols), F32),
            pltpu.VMEM((3, experts, shard, cols), BF16),
            pltpu.VMEM((3, depth, cols), BF16),
            pltpu.VMEM((n_rows, width), BF16),
            pltpu.VMEM((experts, experts, lanes), F32),
            pltpu.VMEM((experts, experts, lanes), F32),
            pltpu.VMEM((n_slots, width), BF16),
            pltpu.VMEM((half, tok_rows, 2 * CAP), BF16),
            pltpu.VMEM((n_slots, 128), F32),
            pltpu.VMEM((n_slots, cols), BF16),
            pltpu.VMEM((n_slots, width), BF16),
            pltpu.VMEM((tps - 1, n_slots, block), BF16),
            pltpu.VMEM((half, CAP, block), BF16),
            pltpu.VMEM((half, 2 * CAP, block), BF16),
            pltpu.VMEM((half * tok_rows, block), BF16),
            pltpu.VMEM(((half - 1) * tok_rows, block), BF16),
            pltpu.VMEM((tok_rows, width), BF16),
            dma((3, experts)),
            dma((3, experts)),
            dma((3, experts)),
            dma((3, experts, copies)),
            dma((3, experts, copies)),
            dma((experts,)),
            dma((experts,)),
            dma((experts,)),
            dma((experts,)),
            dma((experts, tps)),
            dma((experts, tps)),
            dma((experts,)),
            dma((tps - 1, n_w)),
            dma((bits, n_w)),
            dma((bits, n_w)),
            dma((n_w, tps)),
            dma((n_w, tps)),
            dma((3,)),
            dma,
        ],
        compiler_params=pltpu.CompilerParams(
            collective_id=0, has_side_effects=True, vmem_limit_bytes=64 * 1024 * 1024 - 65536
        ),
        name="layer",
    )(
        tokens,
        route_ids.T,
        route_logits.T,
        norm_gain[None, :],
        gate_weight,
        up_weight,
        down_weight,
    )


def solution(mesh):
    return jax.shard_map(
        body,
        mesh=mesh,
        in_specs=(
            P("fs", None),
            P("fs", None),
            P("fs", None),
            P("fs"),
            P(None, "fs", "tp"),
            P(None, "fs", "tp"),
            P(None, "fs", "tp"),
        ),
        out_specs=(P("fs", None), P("fs", None, "tp"), P("fs", None, "tp"), P("fs", None, "tp")),
        check_vma=False,
    )
```

```python
import functools
import math

import jax
import jax.numpy as jnp
from jax import lax
from jax.experimental import pallas as pl
from jax.experimental.pallas import tpu as pltpu
from jax.sharding import PartitionSpec as P

CAP = 96
STORES = 4
PARTS = 1
KERNEL_VMEM = 46 * 1024 * 1024
MESH = pl.DeviceIdType.MESH
BF16 = jnp.bfloat16
F32 = jnp.float32


def layer(
    experts,
    copies,
    tps,
    tokens,
    ids,
    logits,
    gain,
    gate_in,
    up_in,
    down_in,
    mixed,
    gate_full,
    up_full,
    down_full,
    tok,
    gain_col,
    stage,
    send,
    rows_in,
    table,
    rank,
    packed,
    unpack,
    scale,
    hidden,
    part,
    part_in,
    outbox,
    pair,
    share,
    arrived,
    load_sem,
    w_send,
    w_recv,
    r_send,
    r_recv,
    t_send,
    t_recv,
    s_send,
    s_recv,
    tx_send,
    tx_recv,
    p_send,
    p_recv,
    g_send,
    g_recv,
    f_send,
    f_recv,
    tok_sem,
):
    shard, cols = stage.shape[2], stage.shape[3]
    tok_rows, width = tok.shape
    block = width // tps
    chunk_f = min(256, cols)
    chunk_w = width // experts
    n_f, n_w = cols // chunk_f, experts // tps
    bits = experts.bit_length() - 1
    half = experts // 2
    me = lax.axis_index("fs")
    tp = lax.axis_index("tp")
    group = lax.div(me, copies)
    lane = lax.rem(me, copies)
    weights = (gate_in, up_in, down_in)
    full = (gate_full, up_full, down_full)

    def mirror(o):
        return int(f"{o:0{bits}b}"[::-1], 2)

    place = sum(
        lax.rem(lax.div(group, 1 << i), 2) * (1 << (bits - 1 - i)) for i in range(bits)
    )

    at_end = lax.rem(lax.div(group, half), 2) == lax.rem(lax.div(group, half // 2), 2)

    def turn(d):
        swapped = lax.bitwise_xor(jnp.int32(d), jnp.int32(half // 2))
        return lax.select(jnp.logical_and(at_end, d >= half), swapped, jnp.int32(d))

    def ahead(d):
        return lax.bitwise_xor(group, jnp.int32(d))

    def twin(c):
        return lax.rem(lane + c, copies)

    def mate(p):
        return lax.rem(tp + p, tps)

    def kept(k):
        return lax.div(place, 1 << k) * (1 << k)

    def other(k):
        return lax.bitwise_xor(kept(k), jnp.int32(1 << k))

    def hop(k):
        return ahead(experts >> (k + 1)) * copies + lane

    def rows(b, k=0):
        return pl.ds(pl.multiple_of(b * tok_rows, 16), tok_rows << k)

    def slots(b):
        return pl.ds(pl.multiple_of(b * CAP, 16), CAP)

    def own_cols(q):
        return pl.ds(pl.multiple_of(q * block, 128), block)

    n_sub = min(max(chunk_w // 128, 1), copies)
    sub_w, lanes_in = chunk_w // n_sub, copies // n_sub

    def piece(t):
        return lax.rem(lax.div(lane, lanes_in) + t, n_sub)

    def features(e, v=None):
        if v is None:
            return pl.ds(pl.multiple_of(e * chunk_w, 128), chunk_w)
        return pl.ds(pl.multiple_of(e * chunk_w + v * sub_w, 128), sub_w)

    def mark(v):
        return 0 if v is None else v

    def shard_rows(g, c):
        return pl.ds(pl.multiple_of((g * copies + c) * shard, 32), shard)

    def loop(lo, hi, body):
        def step(i, carry):
            body(i)
            return carry

        lax.fori_loop(lo, hi, step, 0)

    def remote(src, dst, s_sem, r_sem, fs_to, tp_to):
        return pltpu.make_async_remote_copy(
            src_ref=src,
            dst_ref=dst,
            send_sem=s_sem,
            recv_sem=r_sem,
            device_id=(fs_to, tp_to),
            device_id_type=MESH,
        )

    def load(m, h):
        return pltpu.make_async_copy(weights[m].at[h], stage.at[m, h], load_sem.at[m, h])

    def half_rows(g, c, r):
        at = (g * copies + c) * shard + r * (shard // PARTS)
        return pl.ds(pl.multiple_of(at, 16), shard // PARTS)

    def direct(m, h, s, r):
        return remote(
            send.at[m, h, pl.ds(r * (shard // PARTS), shard // PARTS)],
            full[m].at[0, half_rows(s, lane, r)],
            w_send.at[m, h, r],
            w_recv.at[m, s, r],
            h * copies + lane,
            tp,
        )

    def relay(m, s, c, to, r):
        return remote(
            full[m].at[0, half_rows(s, c, r)],
            full[m].at[0, half_rows(s, c, r)],
            r_send.at[m, s, to, r],
            r_recv.at[m, s, c, r],
            group * copies + to,
            tp,
        )

    def at_offset(o):
        return lax.bitwise_xor(place, jnp.int32(mirror(o)))

    def gather(o, b):
        span = rows_in.at[rows(at_offset(o)), own_cols(tp)]
        return remote(span, span, t_send.at[o ^ b], t_recv.at[o ^ b], ahead(b) * copies + lane, tp)

    def share_table(o, b):
        span = table.at[at_offset(o)]
        return remote(span, span, s_send.at[o ^ b], s_recv.at[o ^ b], ahead(b) * copies + lane, tp)

    def gather_in(o):
        span, row = rows_in.at[rows(at_offset(o)), own_cols(tp)], table.at[at_offset(o)]
        b = ahead(o & -o) * copies + lane
        remote(span, span, t_send.at[o], t_recv.at[o], b, tp).wait_recv()
        remote(row, row, s_send.at[o], s_recv.at[o], b, tp).wait_recv()

    def spread(o, q, p):
        span = rows_in.at[rows(at_offset(o)), own_cols(q)]
        return remote(span, span, tx_send.at[o, p], tx_recv.at[o, p], me, mate(p))

    def partial(e, v=None):
        owner, j = lax.rem(e, tps), lax.div(e, tps)
        p = lax.rem(owner - tp + tps, tps)
        return remote(
            part.at[:, features(e, v)],
            part_in.at[p - 1, :, features(j, v)],
            p_send.at[e, mark(v)],
            p_recv.at[p - 1, j, mark(v)],
            me,
            owner,
        )

    def partial_in(p, j, v=None):
        span = part_in.at[p - 1, :, features(j, v)]
        return remote(span, span, p_send.at[0, 0], p_recv.at[p - 1, j, mark(v)], me, mate(p))

    def landing(k):
        return pl.ds(((1 << k) - 1) * tok_rows, tok_rows << k)

    def reduce(k, j, v=None):
        if k == bits - 1:
            src = outbox.at[:, :, features(j, v)]
            dst = pair.at[:, pl.ds(CAP, CAP), features(j, v)]
        else:
            src = share.at[rows(other(k) - kept(bits - 1), k), features(j, v)]
            dst = arrived.at[landing(k), features(j, v)]
        return remote(src, dst, g_send.at[k, j, mark(v)], g_recv.at[k, j, mark(v)], hop(k), tp)

    def fan(q, j, p, v=None):
        span = mixed.at[:, features(j * tps + q, v)]
        return remote(
            span, span, f_send.at[j, p, mark(v)], f_recv.at[j, p, mark(v)], me, mate(p)
        )

    tok_copy = pltpu.make_async_copy(tokens, tok, tok_sem)
    tok_copy.start()
    for m in range(3):
        loop(0, experts, lambda d, m=m: load(m, ahead(d)).start())

    barrier = pltpu.get_barrier_semaphore()
    for d in range(1, experts):
        pl.semaphore_signal(
            barrier, inc=1, device_id=(ahead(d) * copies + lane, tp), device_id_type=MESH
        )
    for c in range(1, copies):
        pl.semaphore_signal(
            barrier, inc=1, device_id=(group * copies + twin(c), tp), device_id_type=MESH
        )
    for p in range(1, tps):
        pl.semaphore_signal(barrier, inc=1, device_id=(me, mate(p)), device_id_type=MESH)

    down_rows = lax.broadcasted_iota(jnp.int32, (shard, shard), 0)
    across = lax.broadcasted_iota(jnp.int32, (shard, shard), 1)
    gain_col[...] = jnp.sum(
        jnp.where(down_rows == across, gain[...], 0.0), axis=1, keepdims=True
    )

    gap = logits[0:1, :] - logits[1:2, :]
    choice = (1.0 / (1.0 + jnp.exp(-gap)), 1.0 / (1.0 + jnp.exp(gap)))
    named = lax.broadcasted_iota(jnp.int32, (experts, tok_rows), 0)
    table[place] = jnp.zeros(table.shape[1:], F32)
    table[place, :, 0:tok_rows] = sum(
        jnp.where(ids[k : k + 1, :] == named, choice[k], 0.0) for k in range(2)
    )

    phase = jax.named_scope
    tok_copy.wait()
    step_rows = math.gcd(tok_rows, 32)

    def normalize(i):
        at = pl.multiple_of(i * step_rows, 16)
        values = tok[pl.ds(at, step_rows), :].astype(F32)
        values = values - jnp.mean(values, axis=1, keepdims=True)
        var = jnp.mean(values * values, axis=1, keepdims=True)
        where = pl.ds(pl.multiple_of(place * tok_rows + at, 16), step_rows)
        rows_in[where, :] = (values * lax.rsqrt(var + 1e-06)).astype(BF16)

    loop(0, tok_rows // step_rows, normalize)

    def rounded(m, h):
        load(m, h).wait()
        value = stage[m, h]
        if m < 2:
            value = gain_col[...] * value
        return value.astype(BF16)

    full[0][0, shard_rows(group, lane)] = rounded(0, group)

    with phase("barrier"):
        pl.semaphore_wait(barrier, experts + copies + tps - 3)

    masks = [1 << k for k in range(bits - 1, -1, -1)]

    def forward(o):
        for b in masks:
            if o == 0 or b < o & -o:
                gather(o, b).start()
                share_table(o, b).start()

    forward(0)

    def convert(m, lo, hi):
        def one(d):
            send[m, ahead(d)] = rounded(m, ahead(d))

        loop(lo, hi, one)

    def start(m, lo, hi):
        def one(d):
            for r in range(PARTS):
                direct(m, ahead(d), group, r).start()

        loop(lo, hi, one)

    def relay_own(m):
        for c in range(1, copies):
            for r in range(PARTS):
                relay(m, group, lane, twin(c), r).start()

    def relay_step(m, d):
        s = ahead(turn(d))
        for r in range(PARTS):
            direct(m, s, s, r).wait_recv()
            for c in range(1, copies):
                relay(m, s, lane, twin(c), r).start()

    def relay_wait(m, s):
        for c in range(1, copies):
            for r in range(PARTS):
                relay(m, s, twin(c), lane, r).wait_recv()

    def gathered(o):
        gather_in(o)
        forward(o)
        for p in range(1, tps):
            spread(o, tp, p).start()

    def relays(m, lo, hi):
        loop(lo, hi, lambda d: relay_step(m, d))

    early = half + max(half // 2, 1)
    with phase("first"):
        convert(0, 2, early)
        relay_own(0)
        start(0, 2, early)
        convert(0, 1, 2)
        for m in range(1, 3):
            full[m][0, shard_rows(group, lane)] = rounded(m, group)
            start(m - 1, 1, 2)
            convert(m, 1, 2)
            relay_own(m)
        start(2, 1, 2)
        convert(0, early, experts)
        convert(1, 2, experts)
        convert(2, 2, experts)
    with phase("gate_1"):
        relays(0, 1, 2)
    for o in range(2, half, 2):
        with phase("tok_low"):
            gathered(o)
    with phase("tok_half"):
        gathered(half)
    start(0, early, experts)
    start(1, 2, experts)
    with phase("up_down_1"):
        relays(1, 1, 2)
        relays(2, 1, 2)
    with phase("gate_near"):
        relays(0, 2, half)
    for o in range(half + 2, experts, 2):
        with phase("tok_high"):
            gathered(o)
    start(2, 2, half)
    with phase("gate_far"):
        relays(0, half, experts)
    for o in range(1, experts, 2):
        with phase("tok_odd"):
            gathered(o)

    with phase("gate_wait"):
        for o in range(1, experts):
            for p in range(1, tps):
                spread(o, mate(tps - p), p).wait_recv()

    lanes = table.shape[2]
    before = lax.broadcasted_iota(jnp.int32, (lanes, lanes), 0)
    after = lax.broadcasted_iota(jnp.int32, (lanes, lanes), 1)
    earlier = jnp.where(before < after, 1.0, 0.0).astype(BF16)

    def set_rank(b):
        chosen = table[b] > 0.0
        count = jnp.dot(
            jnp.where(chosen, 1.0, 0.0).astype(BF16), earlier, preferred_element_type=F32
        )
        rank[b] = jnp.where(chosen, count, -4.0 * CAP)

    def pack(b):
        slot = lax.broadcasted_iota(jnp.int32, (CAP, lanes), 0).astype(F32)
        hit = jnp.where(rank[b, pl.ds(group, 1), :] == slot, 1.0, 0.0)
        weight = jnp.sum(hit * table[b, pl.ds(group, 1), :], axis=1, keepdims=True)
        scale[slots(b), :] = jnp.broadcast_to(weight, (CAP, 128))
        packed[slots(b), :] = jnp.dot(
            hit[:, :tok_rows].astype(BF16), rows_in[rows(b), :], preferred_element_type=F32
        ).astype(BF16)

    def column(b, e):
        row = rank[b, pl.ds(e, 1), :]
        return jnp.transpose(jnp.broadcast_to(row, (128, lanes)))[:tok_rows, 0:1]

    def set_unpack(i):
        b = kept(bits - 1) + i
        slot = lax.broadcasted_iota(jnp.int32, (tok_rows, 2 * CAP), 1).astype(F32)
        hit = (column(b, group) == slot) | (column(b, ahead(1)) + CAP == slot)
        unpack[i] = jnp.where(hit, 1.0, 0.0).astype(BF16)

    with phase("set_rank"):
        loop(0, experts, set_rank)
    with phase("pack"):
        loop(0, experts, pack)
    with phase("set_unpack"):
        loop(0, half, set_unpack)

    def project(m, pending):
        def one(c):
            for slot, d in pending:
                @pl.when(c == min(slot, n_f - 1))
                def _():
                    with phase("relay_in"):
                        relay_step(m + 1, d)

            where = pl.ds(pl.multiple_of(c * chunk_f, 128), chunk_f)
            out = jnp.dot(packed[...], full[m][0, :, where], preferred_element_type=F32)
            if m == 0:
                out = out / (1.0 + jnp.exp(-out))
            else:
                out = out * hidden[:, where].astype(F32)
            hidden[:, where] = out.astype(BF16)

        with phase("project"):
            loop(0, n_f, one)

    with phase("gate_wait"):
        loop(0, experts, lambda s: relay_wait(0, s))
    project(0, [(i, 2 + i) for i in range(half)])

    @pl.when(jnp.logical_not(at_end))
    def _():
        start(2, half, experts)

    def directs_sent(m, lo, hi):
        def one(d):
            for r in range(PARTS):
                direct(m, ahead(d), group, r).wait_send()

        loop(lo, hi, one)

    def relays_sent(m, lo, hi):
        def one(d):
            for c in range(1, copies):
                for r in range(PARTS):
                    relay(m, ahead(turn(d)), lane, twin(c), r).wait_send()

        loop(lo, hi, one)

    with phase("sent_0"):
        for o in range(experts):
            for b in masks:
                if o == 0 or b < o & -o:
                    gather(o, b).wait_send()
                    share_table(o, b).wait_send()
            for p in range(1, tps):
                if o:
                    spread(o, tp, p).wait_send()
        directs_sent(0, 1, experts)
        relays_sent(0, 0, experts)
    with phase("up_rest"):
        relays(1, 2 + half, experts)

    with phase("up_wait"):
        loop(0, experts, lambda s: relay_wait(1, s))

    @pl.when(at_end)
    def _():
        start(2, half, experts)

    project(1, [(2 * i, 2 + i) for i in range(half - 2)])

    def add_up(d, v=None):
        e = ahead(turn(d))

        @pl.when(lax.rem(e, tps) == tp)
        def _():
            j = lax.div(e, tps)
            for p in range(1, tps):
                partial_in(p, j, v).wait_recv()
            wide = chunk_w if v is None else sub_w
            step = min(wide, 128)
            skip = 0 if v is None else v * sub_w

            def fill(target, first):
                def one(i):
                    b = first + i
                    for q in range(0, wide, step):
                        here = pl.ds(pl.multiple_of(e * chunk_w + skip + q, step), step)
                        there = pl.ds(pl.multiple_of(j * chunk_w + skip + q, step), step)
                        total = part[slots(b), here].astype(F32)
                        for p in range(1, tps):
                            total = total + part_in[p - 1, slots(b), there].astype(F32)
                        target[i, 0:CAP, there] = (scale[slots(b), 0:step] * total).astype(BF16)

                loop(0, half, one)

            fill(outbox, other(bits - 1))
            reduce(bits - 1, j, v).start()
            fill(pair, kept(bits - 1))

    def down_step(d, v=None):
        e = ahead(turn(d))
        if v is None:
            relay_wait(2, e)
        else:
            for c in range(lanes_in):
                source = v * lanes_in + c

                @pl.when(source != lane)
                def _():
                    for r in range(PARTS):
                        relay(2, e, source, lane, r).wait_recv()

        part[:, features(e, v)] = lax.dot_general(
            hidden[...],
            full[2][0, features(e, v), :],
            (((1,), (1,)), ((), ())),
            preferred_element_type=F32,
        ).astype(BF16)

        @pl.when(lax.rem(e, tps) != tp)
        def _():
            partial(e, v).start()

    def owned(i, q):
        d = tps * i + lax.bitwise_xor(q, lax.rem(group, tps))
        return lax.div(ahead(turn(d)), tps)

    def reduce_step(k, i, v=None, onward=True):
        j = owned(i, tp)
        reduce(k, j, v).wait_recv()
        base = kept(k) - kept(bits - 1)

        def one(b):
            here = rows(base + b)
            if k == bits - 1:
                total = jnp.dot(unpack[b], pair[b, :, features(j, v)], preferred_element_type=F32)
            else:
                come = pl.ds(pl.multiple_of(((1 << k) - 1 + b) * tok_rows, 16), tok_rows)
                total = share[here, features(j, v)].astype(F32)
                total = total + arrived[come, features(j, v)].astype(F32)
            if k > 0:
                share[here, features(j, v)] = total.astype(BF16)
            else:
                mixed[:, features(j * tps + tp, v)] = total.astype(BF16)

        loop(0, 1 << k, one)
        if k > 0 and onward:
            reduce(k - 1, j, v).start()
        if k == 0:
            for p in range(1, tps):
                fan(tp, j, p, v).start()

    def add_ups(lo, hi, v=None):
        with phase("add"):
            loop(lo, hi, lambda d: add_up(d, v))

    def down_steps(lo, hi, v=None):
        with phase("down"):
            loop(lo, hi, lambda d: down_step(d, v))

    def reduce_steps(k, lo, hi, v=None, onward=True):
        with phase(f"reduce{k}"):
            loop(lo, hi, lambda i: reduce_step(k, i, v, onward))

    def relay_early():
        with phase("relay_early"):
            relays(2, half, early)

    near_w = n_w // 2
    early_w = near_w + near_w // 2
    later = early + (experts - early) // 2
    pieces = [piece(t) for t in range(n_sub)]
    near_pieces = [None] if near_w else pieces

    for v in near_pieces:
        def near_step(d, v=v):
            down_step(d, v)

            @pl.when(d > 0)
            def _():
                add_up(d - 1, v)

        with phase("near"):
            loop(0, half, near_step)
        add_ups(half - 1, half, v)
    pl.when(jnp.logical_not(at_end))(relay_early)
    with phase("sent_1"):
        directs_sent(1, 1, experts)
        relays_sent(1, 0, experts)
        directs_sent(2, 1, half)
    reduce_steps(bits - 1, 0, near_w)
    pl.when(at_end)(relay_early)
    for v in pieces:
        down_steps(half, early, v)
    for v in pieces:
        add_ups(half, early, v)
    with phase("relay_6"):
        relays(2, early, later)

    def relay_last():
        with phase("relay_7"):
            relays(2, later, experts)

    pl.when(at_end)(relay_last)
    for k in range(bits - 2, 0, -1):
        reduce_steps(k, 0, near_w, onward=k > 1)
    for v in pieces:
        reduce_steps(bits - 1, near_w, early_w, v)
    down_steps(early, later, pieces[0])
    pl.when(jnp.logical_not(at_end))(relay_last)
    down_steps(later, experts, pieces[0])
    loop(0, near_w, lambda i: reduce(0, owned(i, tp)).start())
    add_ups(early, experts, pieces[0])
    for k in range(bits - 2, 0, -1):
        for v in pieces:
            reduce_steps(k, near_w, early_w, v)
    for v in pieces[1:]:
        down_steps(early, experts, v)
    for v in pieces[1:]:
        add_ups(early, experts, v)
    for k in range(bits - 1, 0, -1):
        for v in pieces:
            reduce_steps(k, early_w, n_w, v)
    def part_sent(d, v=None):
        @pl.when(lax.rem(ahead(d), tps) != tp)
        def _():
            partial(ahead(d), v).wait_send()

    with phase("sent_2"):
        directs_sent(2, half, experts)
        relays_sent(2, 0, experts)
        for v in near_pieces:
            loop(0, half, lambda d, v=v: part_sent(d, v))
        for v in pieces:
            loop(half, experts, lambda d, v=v: part_sent(d, v))
        for k in range(1, bits):
            loop(0, near_w, lambda i, k=k: reduce(k, owned(i, tp)).wait_send())
            for v in pieces:
                loop(near_w, n_w, lambda i, k=k, v=v: reduce(k, owned(i, tp), v).wait_send())
    with phase("last_far"):
        for v in near_pieces:
            loop(near_w, n_w, lambda i, v=v: reduce_step(0, i, v))
    with phase("last_near"):
        for v in pieces:
            loop(0, near_w, lambda i, v=v: reduce_step(0, i, v))

    with phase("fan_wait"):
        for p in range(1, tps):
            q = mate(tps - p)
            for v in near_pieces:
                loop(near_w, n_w, lambda i, p=p, q=q, v=v: fan(q, owned(i, q), p, v).wait_recv())
            for v in pieces:
                loop(0, near_w, lambda i, p=p, q=q, v=v: fan(q, owned(i, q), p, v).wait_recv())
    loop(0, near_w, lambda i: reduce(0, owned(i, tp)).wait_send())
    for v in pieces:
        loop(near_w, n_w, lambda i, v=v: reduce(0, owned(i, tp), v).wait_send())
    for p in range(1, tps):
        for v in near_pieces:
            loop(near_w, n_w, lambda i, p=p, v=v: fan(tp, owned(i, tp), p, v).wait_send())
        for v in pieces:
            loop(0, near_w, lambda i, p=p, v=v: fan(tp, owned(i, tp), p, v).wait_send())


def store(*refs):
    copies = [pltpu.make_async_copy(refs[0], refs[4], refs[-1].at[0, 0])]
    for i in range(1, 4):
        size = refs[i].shape[1] // STORES
        for k in range(STORES):
            at = (slice(None), pl.ds(k * size, size))
            copies.append(pltpu.make_async_copy(refs[i].at[at], refs[4 + i].at[at], refs[-1].at[i, k]))
    for copy in copies:
        copy.start()
    for copy in copies:
        copy.wait()


def body(tokens, route_ids, route_logits, norm_gain, gate_weight, up_weight, down_weight):
    experts, shard, cols = gate_weight.shape
    fs_count, tps = lax.axis_size("fs"), lax.axis_size("tp")
    copies = fs_count // experts
    tok_rows, width = tokens.shape
    block = width // tps
    n_rows, n_slots = experts * tok_rows, experts * CAP
    lanes, half = -(-tok_rows // 128) * 128, experts // 2
    n_sub = min(max(width // experts // 128, 1), copies)
    assert copies % n_sub == 0
    depth = shard * fs_count
    n_w = experts // tps
    bits = experts.bit_length() - 1
    assert experts == 1 << bits and bits > 1
    assert tps & (tps - 1) == 0 and n_w * tps == experts

    dma = pltpu.SemaphoreType.DMA
    anywhere = pl.BlockSpec(memory_space=pl.ANY)
    inside = pl.BlockSpec(memory_space=pltpu.VMEM)
    shapes = ((tok_rows, width),) + ((1, depth, cols),) * 3
    results = pl.pallas_call(
        functools.partial(layer, experts, copies, tps),
        out_shape=tuple(pltpu.VMEM(shape, BF16) for shape in shapes),
        in_specs=[anywhere] + [inside] * 3 + [anywhere] * 3,
        out_specs=(inside,) * 4,
        scratch_shapes=[
            pltpu.VMEM((tok_rows, width), BF16),
            pltpu.VMEM((shard, 1), F32),
            pltpu.VMEM((3, experts, shard, cols), F32),
            pltpu.VMEM((3, experts, shard, cols), BF16),
            pltpu.VMEM((n_rows, width), BF16),
            pltpu.VMEM((experts, experts, lanes), F32),
            pltpu.VMEM((experts, experts, lanes), F32),
            pltpu.VMEM((n_slots, width), BF16),
            pltpu.VMEM((half, tok_rows, 2 * CAP), BF16),
            pltpu.VMEM((n_slots, 128), F32),
            pltpu.VMEM((n_slots, cols), BF16),
            pltpu.VMEM((n_slots, width), BF16),
            pltpu.VMEM((tps - 1, n_slots, block), BF16),
            pltpu.VMEM((half, CAP, block), BF16),
            pltpu.VMEM((half, 2 * CAP, block), BF16),
            pltpu.VMEM((half * tok_rows, block), BF16),
            pltpu.VMEM(((half - 1) * tok_rows, block), BF16),
            dma((3, experts)),
            dma((3, experts, PARTS)),
            dma((3, experts, PARTS)),
            dma((3, experts, copies, PARTS)),
            dma((3, experts, copies, PARTS)),
            dma((experts,)),
            dma((experts,)),
            dma((experts,)),
            dma((experts,)),
            dma((experts, tps)),
            dma((experts, tps)),
            dma((experts, n_sub)),
            dma((tps - 1, n_w, n_sub)),
            dma((bits, n_w, n_sub)),
            dma((bits, n_w, n_sub)),
            dma((n_w, tps, n_sub)),
            dma((n_w, tps, n_sub)),
            dma,
        ],
        compiler_params=pltpu.CompilerParams(
            collective_id=0, has_side_effects=True, vmem_limit_bytes=KERNEL_VMEM
        ),
        name="layer",
    )(
        tokens,
        route_ids.T,
        route_logits.T,
        norm_gain[None, :],
        gate_weight,
        up_weight,
        down_weight,
    )
    return pl.pallas_call(
        store,
        out_shape=tuple(jax.ShapeDtypeStruct(shape, BF16) for shape in shapes),
        in_specs=[inside] * 4,
        out_specs=(anywhere,) * 4,
        scratch_shapes=[dma((4, STORES))],
        compiler_params=pltpu.CompilerParams(vmem_limit_bytes=1024 * 1024),
        name="store",
    )(*results)


def solution(mesh):
    return jax.shard_map(
        body,
        mesh=mesh,
        in_specs=(
            P("fs", None),
            P("fs", None),
            P("fs", None),
            P("fs"),
            P(None, "fs", "tp"),
            P(None, "fs", "tp"),
            P(None, "fs", "tp"),
        ),
        out_specs=(P("fs", None), P("fs", None, "tp"), P("fs", None, "tp"), P("fs", None, "tp")),
        check_vma=False,
    )
```

```python
import functools
import math

import jax
import jax.numpy as jnp
from jax import lax
from jax.experimental import pallas as pl
from jax.experimental.pallas import tpu as pltpu
from jax.sharding import PartitionSpec as P

CAP = 96
STORES = 4
PARTS = 1
KERNEL_VMEM = 46 * 1024 * 1024
MESH = pl.DeviceIdType.MESH
BF16 = jnp.bfloat16
F32 = jnp.float32


def layer(
    experts,
    copies,
    tps,
    tokens,
    ids,
    logits,
    gain,
    gate_in,
    up_in,
    down_in,
    mixed,
    gate_full,
    up_full,
    down_full,
    tok,
    gain_col,
    stage,
    send,
    rows_in,
    table,
    rank,
    packed,
    unpack,
    scale,
    hidden,
    part,
    part_in,
    outbox,
    pair,
    share,
    arrived,
    load_sem,
    w_send,
    w_recv,
    r_send,
    r_recv,
    t_send,
    t_recv,
    s_send,
    s_recv,
    tx_send,
    tx_recv,
    p_send,
    p_recv,
    g_send,
    g_recv,
    f_send,
    f_recv,
    tok_sem,
):
    shard, cols = stage.shape[2], stage.shape[3]
    tok_rows, width = tok.shape
    block = width // tps
    chunk_f = min(256, cols)
    chunk_w = width // experts
    n_f, n_w = cols // chunk_f, experts // tps
    bits = experts.bit_length() - 1
    half = experts // 2
    me = lax.axis_index("fs")
    tp = lax.axis_index("tp")
    group = lax.div(me, copies)
    lane = lax.rem(me, copies)
    weights = (gate_in, up_in, down_in)
    full = (gate_full, up_full, down_full)

    def mirror(o):
        return int(f"{o:0{bits}b}"[::-1], 2)

    place = sum(
        lax.rem(lax.div(group, 1 << i), 2) * (1 << (bits - 1 - i)) for i in range(bits)
    )

    at_end = lax.rem(lax.div(group, half), 2) == lax.rem(lax.div(group, half // 2), 2)

    def turn(d):
        swapped = lax.bitwise_xor(jnp.int32(d), jnp.int32(half // 2))
        return lax.select(jnp.logical_and(at_end, d >= half), swapped, jnp.int32(d))

    def ahead(d):
        return lax.bitwise_xor(group, jnp.int32(d))

    def twin(c):
        return lax.rem(lane + c, copies)

    def mate(p):
        return lax.rem(tp + p, tps)

    def kept(k):
        return lax.div(place, 1 << k) * (1 << k)

    def other(k):
        return lax.bitwise_xor(kept(k), jnp.int32(1 << k))

    def hop(k):
        return ahead(experts >> (k + 1)) * copies + lane

    def rows(b, k=0):
        return pl.ds(pl.multiple_of(b * tok_rows, 16), tok_rows << k)

    def slots(b):
        return pl.ds(pl.multiple_of(b * CAP, 16), CAP)

    def own_cols(q):
        return pl.ds(pl.multiple_of(q * block, 128), block)

    n_sub = min(max(chunk_w // 128, 1), copies)
    sub_w, lanes_in = chunk_w // n_sub, copies // n_sub

    def piece(t):
        return lax.rem(lax.div(lane, lanes_in) + t, n_sub)

    def features(e, v=None):
        if v is None:
            return pl.ds(pl.multiple_of(e * chunk_w, 128), chunk_w)
        return pl.ds(pl.multiple_of(e * chunk_w + v * sub_w, 128), sub_w)

    def mark(v):
        return 0 if v is None else v

    def shard_rows(g, c):
        return pl.ds(pl.multiple_of((g * copies + c) * shard, 32), shard)

    def loop(lo, hi, body):
        def step(i, carry):
            body(i)
            return carry

        lax.fori_loop(lo, hi, step, 0)

    def remote(src, dst, s_sem, r_sem, fs_to, tp_to):
        return pltpu.make_async_remote_copy(
            src_ref=src,
            dst_ref=dst,
            send_sem=s_sem,
            recv_sem=r_sem,
            device_id=(fs_to, tp_to),
            device_id_type=MESH,
        )

    def load(m, h):
        return pltpu.make_async_copy(weights[m].at[h], stage.at[m, h], load_sem.at[m, h])

    def half_rows(g, c, r):
        at = (g * copies + c) * shard + r * (shard // PARTS)
        return pl.ds(pl.multiple_of(at, 16), shard // PARTS)

    def direct(m, h, s, r):
        return remote(
            send.at[m, h, pl.ds(r * (shard // PARTS), shard // PARTS)],
            full[m].at[0, half_rows(s, lane, r)],
            w_send.at[m, h, r],
            w_recv.at[m, s, r],
            h * copies + lane,
            tp,
        )

    def relay(m, s, c, to, r):
        return remote(
            full[m].at[0, half_rows(s, c, r)],
            full[m].at[0, half_rows(s, c, r)],
            r_send.at[m, s, to, r],
            r_recv.at[m, s, c, r],
            group * copies + to,
            tp,
        )

    def at_offset(o):
        return lax.bitwise_xor(place, jnp.int32(mirror(o)))

    def gather(o, b):
        span = rows_in.at[rows(at_offset(o)), own_cols(tp)]
        return remote(span, span, t_send.at[o ^ b], t_recv.at[o ^ b], ahead(b) * copies + lane, tp)

    def share_table(o, b):
        span = table.at[at_offset(o)]
        return remote(span, span, s_send.at[o ^ b], s_recv.at[o ^ b], ahead(b) * copies + lane, tp)

    def gather_in(o):
        span, row = rows_in.at[rows(at_offset(o)), own_cols(tp)], table.at[at_offset(o)]
        b = ahead(o & -o) * copies + lane
        remote(span, span, t_send.at[o], t_recv.at[o], b, tp).wait_recv()
        remote(row, row, s_send.at[o], s_recv.at[o], b, tp).wait_recv()

    def spread(o, q, p):
        span = rows_in.at[rows(at_offset(o)), own_cols(q)]
        return remote(span, span, tx_send.at[o, p], tx_recv.at[o, p], me, mate(p))

    def partial(e, v=None):
        owner, j = lax.rem(e, tps), lax.div(e, tps)
        p = lax.rem(owner - tp + tps, tps)
        return remote(
            part.at[:, features(e, v)],
            part_in.at[p - 1, :, features(j, v)],
            p_send.at[e, mark(v)],
            p_recv.at[p - 1, j, mark(v)],
            me,
            owner,
        )

    def partial_in(p, j, v=None):
        span = part_in.at[p - 1, :, features(j, v)]
        return remote(span, span, p_send.at[0, 0], p_recv.at[p - 1, j, mark(v)], me, mate(p))

    def landing(k):
        return pl.ds(((1 << k) - 1) * tok_rows, tok_rows << k)

    def reduce(k, j, v=None):
        if k == bits - 1:
            src = outbox.at[:, :, features(j, v)]
            dst = pair.at[:, pl.ds(CAP, CAP), features(j, v)]
        else:
            src = share.at[rows(other(k) - kept(bits - 1), k), features(j, v)]
            dst = arrived.at[landing(k), features(j, v)]
        return remote(src, dst, g_send.at[k, j, mark(v)], g_recv.at[k, j, mark(v)], hop(k), tp)

    def fan(q, j, p, v=None):
        span = mixed.at[:, features(j * tps + q, v)]
        return remote(
            span, span, f_send.at[j, p, mark(v)], f_recv.at[j, p, mark(v)], me, mate(p)
        )

    tok_copy = pltpu.make_async_copy(tokens, tok, tok_sem)
    tok_copy.start()
    for m in range(3):
        loop(0, experts, lambda d, m=m: load(m, ahead(d)).start())

    barrier = pltpu.get_barrier_semaphore()
    for d in range(1, experts):
        pl.semaphore_signal(
            barrier, inc=1, device_id=(ahead(d) * copies + lane, tp), device_id_type=MESH
        )
    for c in range(1, copies):
        pl.semaphore_signal(
            barrier, inc=1, device_id=(group * copies + twin(c), tp), device_id_type=MESH
        )
    for p in range(1, tps):
        pl.semaphore_signal(barrier, inc=1, device_id=(me, mate(p)), device_id_type=MESH)

    down_rows = lax.broadcasted_iota(jnp.int32, (shard, shard), 0)
    across = lax.broadcasted_iota(jnp.int32, (shard, shard), 1)
    gain_col[...] = jnp.sum(
        jnp.where(down_rows == across, gain[...], 0.0), axis=1, keepdims=True
    )

    gap = logits[0:1, :] - logits[1:2, :]
    choice = (1.0 / (1.0 + jnp.exp(-gap)), 1.0 / (1.0 + jnp.exp(gap)))
    named = lax.broadcasted_iota(jnp.int32, (experts, tok_rows), 0)
    table[place] = jnp.zeros(table.shape[1:], F32)
    table[place, :, 0:tok_rows] = sum(
        jnp.where(ids[k : k + 1, :] == named, choice[k], 0.0) for k in range(2)
    )

    phase = jax.named_scope
    tok_copy.wait()
    step_rows = math.gcd(tok_rows, 32)

    def normalize(i):
        at = pl.multiple_of(i * step_rows, 16)
        values = tok[pl.ds(at, step_rows), :].astype(F32)
        values = values - jnp.mean(values, axis=1, keepdims=True)
        var = jnp.mean(values * values, axis=1, keepdims=True)
        where = pl.ds(pl.multiple_of(place * tok_rows + at, 16), step_rows)
        rows_in[where, :] = (values * lax.rsqrt(var + 1e-06)).astype(BF16)

    loop(0, tok_rows // step_rows, normalize)

    def rounded(m, h):
        load(m, h).wait()
        value = stage[m, h]
        if m < 2:
            value = gain_col[...] * value
        return value.astype(BF16)

    full[0][0, shard_rows(group, lane)] = rounded(0, group)

    with phase("barrier"):
        pl.semaphore_wait(barrier, experts + copies + tps - 3)

    masks = [1 << k for k in range(bits - 1, -1, -1)]

    def forward(o):
        for b in masks:
            if o == 0 or b < o & -o:
                gather(o, b).start()
                share_table(o, b).start()

    forward(0)

    def convert(m, lo, hi):
        def one(d):
            send[m, ahead(d)] = rounded(m, ahead(d))

        loop(lo, hi, one)

    def start(m, lo, hi):
        def one(d):
            for r in range(PARTS):
                direct(m, ahead(d), group, r).start()

        loop(lo, hi, one)

    def relay_own(m):
        for c in range(1, copies):
            for r in range(PARTS):
                relay(m, group, lane, twin(c), r).start()

    def relay_step(m, d):
        s = ahead(turn(d))
        for r in range(PARTS):
            direct(m, s, s, r).wait_recv()
            for c in range(1, copies):
                relay(m, s, lane, twin(c), r).start()

    def relay_wait(m, s):
        for c in range(1, copies):
            for r in range(PARTS):
                relay(m, s, twin(c), lane, r).wait_recv()

    def gathered(o):
        gather_in(o)
        forward(o)
        for p in range(1, tps):
            spread(o, tp, p).start()

    def relays(m, lo, hi):
        loop(lo, hi, lambda d: relay_step(m, d))

    early = half + max(half // 2, 1)
    with phase("first"):
        convert(0, 2, early)
        relay_own(0)
        start(0, 2, early)
        convert(0, 1, 2)
        for m in range(1, 3):
            full[m][0, shard_rows(group, lane)] = rounded(m, group)
            start(m - 1, 1, 2)
            convert(m, 1, 2)
            relay_own(m)
        start(2, 1, 2)
        convert(0, early, experts)
        convert(1, 2, experts)
        convert(2, 2, experts)
    with phase("gate_1"):
        relays(0, 1, 2)
    for o in range(2, half, 2):
        with phase("tok_low"):
            gathered(o)
    with phase("tok_half"):
        gathered(half)
    start(0, early, experts)
    start(1, 2, experts)
    with phase("up_down_1"):
        relays(1, 1, 2)
        relays(2, 1, 2)
    with phase("gate_near"):
        relays(0, 2, half)
    for o in range(half + 2, experts, 2):
        with phase("tok_high"):
            gathered(o)
    start(2, 2, half)
    with phase("gate_far"):
        relays(0, half, experts)
    for o in range(1, experts, 2):
        with phase("tok_odd"):
            gathered(o)

    with phase("gate_wait"):
        for o in range(1, experts):
            for p in range(1, tps):
                spread(o, mate(tps - p), p).wait_recv()

    lanes = table.shape[2]
    before = lax.broadcasted_iota(jnp.int32, (lanes, lanes), 0)
    after = lax.broadcasted_iota(jnp.int32, (lanes, lanes), 1)
    earlier = jnp.where(before < after, 1.0, 0.0).astype(BF16)

    def set_rank(b):
        chosen = table[b] > 0.0
        count = jnp.dot(
            jnp.where(chosen, 1.0, 0.0).astype(BF16), earlier, preferred_element_type=F32
        )
        rank[b] = jnp.where(chosen, count, -4.0 * CAP)

    def pack(b):
        slot = lax.broadcasted_iota(jnp.int32, (CAP, lanes), 0).astype(F32)
        hit = jnp.where(rank[b, pl.ds(group, 1), :] == slot, 1.0, 0.0)
        weight = jnp.sum(hit * table[b, pl.ds(group, 1), :], axis=1, keepdims=True)
        scale[slots(b), :] = jnp.broadcast_to(weight, (CAP, 128))
        packed[slots(b), :] = jnp.dot(
            hit[:, :tok_rows].astype(BF16), rows_in[rows(b), :], preferred_element_type=F32
        ).astype(BF16)

    def column(b, e):
        row = rank[b, pl.ds(e, 1), :]
        return jnp.transpose(jnp.broadcast_to(row, (128, lanes)))[:tok_rows, 0:1]

    def set_unpack(i):
        b = kept(bits - 1) + i
        slot = lax.broadcasted_iota(jnp.int32, (tok_rows, 2 * CAP), 1).astype(F32)
        hit = (column(b, group) == slot) | (column(b, ahead(1)) + CAP == slot)
        unpack[i] = jnp.where(hit, 1.0, 0.0).astype(BF16)

    with phase("set_rank"):
        loop(0, experts, set_rank)
    with phase("pack"):
        loop(0, experts, pack)
    with phase("set_unpack"):
        loop(0, half, set_unpack)

    def project(m, pending):
        def one(c):
            for slot, d in pending:
                @pl.when(c == min(slot, n_f - 1))
                def _():
                    with phase("relay_in"):
                        relay_step(m + 1, d)

            where = pl.ds(pl.multiple_of(c * chunk_f, 128), chunk_f)
            out = jnp.dot(packed[...], full[m][0, :, where], preferred_element_type=F32)
            if m == 0:
                out = out / (1.0 + jnp.exp(-out))
            else:
                out = out * hidden[:, where].astype(F32)
            hidden[:, where] = out.astype(BF16)

        with phase("project"):
            loop(0, n_f, one)

    with phase("gate_wait"):
        loop(0, experts, lambda s: relay_wait(0, s))
    project(0, [(i, 2 + i) for i in range(half)])

    @pl.when(jnp.logical_not(at_end))
    def _():
        start(2, half, early)

    def directs_sent(m, lo, hi):
        def one(d):
            for r in range(PARTS):
                direct(m, ahead(d), group, r).wait_send()

        loop(lo, hi, one)

    def relays_sent(m, lo, hi):
        def one(d):
            for c in range(1, copies):
                for r in range(PARTS):
                    relay(m, ahead(turn(d)), lane, twin(c), r).wait_send()

        loop(lo, hi, one)

    with phase("sent_0"):
        for o in range(experts):
            for b in masks:
                if o == 0 or b < o & -o:
                    gather(o, b).wait_send()
                    share_table(o, b).wait_send()
            for p in range(1, tps):
                if o:
                    spread(o, tp, p).wait_send()
        directs_sent(0, 1, experts)
        relays_sent(0, 0, experts)
    with phase("up_rest"):
        relays(1, 2 + half, experts)

    with phase("up_wait"):
        loop(0, experts, lambda s: relay_wait(1, s))

    project(1, [(2 * i, 2 + i) for i in range(half - 2)])

    @pl.when(at_end)
    def _():
        start(2, half, experts)


    def add_up(d, v=None):
        e = ahead(turn(d))

        @pl.when(lax.rem(e, tps) == tp)
        def _():
            j = lax.div(e, tps)
            for p in range(1, tps):
                partial_in(p, j, v).wait_recv()
            wide = chunk_w if v is None else sub_w
            step = min(wide, 128)
            skip = 0 if v is None else v * sub_w

            def fill(target, first):
                def one(i):
                    b = first + i
                    for q in range(0, wide, step):
                        here = pl.ds(pl.multiple_of(e * chunk_w + skip + q, step), step)
                        there = pl.ds(pl.multiple_of(j * chunk_w + skip + q, step), step)
                        total = part[slots(b), here].astype(F32)
                        for p in range(1, tps):
                            total = total + part_in[p - 1, slots(b), there].astype(F32)
                        target[i, 0:CAP, there] = (scale[slots(b), 0:step] * total).astype(BF16)

                loop(0, half, one)

            fill(outbox, other(bits - 1))
            reduce(bits - 1, j, v).start()
            fill(pair, kept(bits - 1))

    def down_step(d, v=None):
        e = ahead(turn(d))
        if v is None:
            relay_wait(2, e)
        else:
            for c in range(lanes_in):
                source = v * lanes_in + c

                @pl.when(source != lane)
                def _():
                    for r in range(PARTS):
                        relay(2, e, source, lane, r).wait_recv()

        part[:, features(e, v)] = lax.dot_general(
            hidden[...],
            full[2][0, features(e, v), :],
            (((1,), (1,)), ((), ())),
            preferred_element_type=F32,
        ).astype(BF16)

        @pl.when(lax.rem(e, tps) != tp)
        def _():
            partial(e, v).start()

    def owned(i, q):
        d = tps * i + lax.bitwise_xor(q, lax.rem(group, tps))
        return lax.div(ahead(turn(d)), tps)

    def reduce_step(k, i, v=None, onward=True):
        j = owned(i, tp)
        reduce(k, j, v).wait_recv()
        base = kept(k) - kept(bits - 1)

        def one(b):
            here = rows(base + b)
            if k == bits - 1:
                total = jnp.dot(unpack[b], pair[b, :, features(j, v)], preferred_element_type=F32)
            else:
                come = pl.ds(pl.multiple_of(((1 << k) - 1 + b) * tok_rows, 16), tok_rows)
                total = share[here, features(j, v)].astype(F32)
                total = total + arrived[come, features(j, v)].astype(F32)
            if k > 0:
                share[here, features(j, v)] = total.astype(BF16)
            else:
                mixed[:, features(j * tps + tp, v)] = total.astype(BF16)

        loop(0, 1 << k, one)
        if k > 0 and onward:
            reduce(k - 1, j, v).start()
        if k == 0:
            for p in range(1, tps):
                fan(tp, j, p, v).start()

    def add_ups(lo, hi, v=None):
        with phase("add"):
            loop(lo, hi, lambda d: add_up(d, v))

    def down_steps(lo, hi, v=None):
        with phase("down"):
            loop(lo, hi, lambda d: down_step(d, v))

    def reduce_steps(k, lo, hi, v=None, onward=True):
        with phase(f"reduce{k}"):
            loop(lo, hi, lambda i: reduce_step(k, i, v, onward))

    def relay_early():
        with phase("relay_early"):
            relays(2, half, early)

    near_w = n_w // 2
    early_w = near_w + near_w // 2
    later = early + (experts - early) // 2
    pieces = [piece(t) for t in range(n_sub)]
    near_pieces = [None] if near_w else pieces

    for v in near_pieces:
        def near_step(d, v=v):
            down_step(d, v)

            @pl.when(d > 0)
            def _():
                add_up(d - 1, v)

        with phase("near"):
            loop(0, half, near_step)
        add_ups(half - 1, half, v)
    pl.when(jnp.logical_not(at_end))(relay_early)
    @pl.when(jnp.logical_not(at_end))
    def _():
        start(2, early, experts)

    with phase("sent_1"):
        directs_sent(1, 1, experts)
        relays_sent(1, 0, experts)
        directs_sent(2, 1, half)
    reduce_steps(bits - 1, 0, near_w)
    pl.when(at_end)(relay_early)
    for v in pieces:
        down_steps(half, early, v)
    for v in pieces:
        add_ups(half, early, v)
    with phase("relay_6"):
        relays(2, early, later)

    def relay_last():
        with phase("relay_7"):
            relays(2, later, experts)

    pl.when(at_end)(relay_last)
    for k in range(bits - 2, 0, -1):
        reduce_steps(k, 0, near_w, onward=k > 1)
    for v in pieces:
        reduce_steps(bits - 1, near_w, early_w, v)
    down_steps(early, later, pieces[0])
    loop(0, near_w, lambda i: reduce(0, owned(i, tp)).start())
    pl.when(jnp.logical_not(at_end))(relay_last)
    down_steps(later, experts, pieces[0])
    add_ups(early, experts, pieces[0])
    for k in range(bits - 2, 0, -1):
        for v in pieces:
            reduce_steps(k, near_w, early_w, v)
    for v in pieces[1:]:
        down_steps(early, experts, v)
    for v in pieces[1:]:
        add_ups(early, experts, v)
    for k in range(bits - 1, 0, -1):
        for v in pieces:
            reduce_steps(k, early_w, n_w, v)
    def part_sent(d, v=None):
        @pl.when(lax.rem(ahead(d), tps) != tp)
        def _():
            partial(ahead(d), v).wait_send()

    with phase("sent_2"):
        directs_sent(2, half, experts)
        relays_sent(2, 0, experts)
        for v in near_pieces:
            loop(0, half, lambda d, v=v: part_sent(d, v))
        for v in pieces:
            loop(half, experts, lambda d, v=v: part_sent(d, v))
        for k in range(1, bits):
            loop(0, near_w, lambda i, k=k: reduce(k, owned(i, tp)).wait_send())
            for v in pieces:
                loop(near_w, n_w, lambda i, k=k, v=v: reduce(k, owned(i, tp), v).wait_send())
    with phase("last_far"):
        for v in near_pieces:
            loop(near_w, n_w, lambda i, v=v: reduce_step(0, i, v))
    with phase("last_near"):
        for v in pieces:
            loop(0, near_w, lambda i, v=v: reduce_step(0, i, v))

    with phase("fan_wait"):
        for p in range(1, tps):
            q = mate(tps - p)
            for v in near_pieces:
                loop(near_w, n_w, lambda i, p=p, q=q, v=v: fan(q, owned(i, q), p, v).wait_recv())
            for v in pieces:
                loop(0, near_w, lambda i, p=p, q=q, v=v: fan(q, owned(i, q), p, v).wait_recv())
    loop(0, near_w, lambda i: reduce(0, owned(i, tp)).wait_send())
    for v in pieces:
        loop(near_w, n_w, lambda i, v=v: reduce(0, owned(i, tp), v).wait_send())
    for p in range(1, tps):
        for v in near_pieces:
            loop(near_w, n_w, lambda i, p=p, v=v: fan(tp, owned(i, tp), p, v).wait_send())
        for v in pieces:
            loop(0, near_w, lambda i, p=p, v=v: fan(tp, owned(i, tp), p, v).wait_send())


def store(*refs):
    copies = [pltpu.make_async_copy(refs[0], refs[4], refs[-1].at[0, 0])]
    for i in range(1, 4):
        size = refs[i].shape[1] // STORES
        for k in range(STORES):
            at = (slice(None), pl.ds(k * size, size))
            copies.append(pltpu.make_async_copy(refs[i].at[at], refs[4 + i].at[at], refs[-1].at[i, k]))
    for copy in copies:
        copy.start()
    for copy in copies:
        copy.wait()


def body(tokens, route_ids, route_logits, norm_gain, gate_weight, up_weight, down_weight):
    experts, shard, cols = gate_weight.shape
    fs_count, tps = lax.axis_size("fs"), lax.axis_size("tp")
    copies = fs_count // experts
    tok_rows, width = tokens.shape
    block = width // tps
    n_rows, n_slots = experts * tok_rows, experts * CAP
    lanes, half = -(-tok_rows // 128) * 128, experts // 2
    n_sub = min(max(width // experts // 128, 1), copies)
    assert copies % n_sub == 0
    depth = shard * fs_count
    n_w = experts // tps
    bits = experts.bit_length() - 1
    assert experts == 1 << bits and bits > 1
    assert tps & (tps - 1) == 0 and n_w * tps == experts

    dma = pltpu.SemaphoreType.DMA
    anywhere = pl.BlockSpec(memory_space=pl.ANY)
    inside = pl.BlockSpec(memory_space=pltpu.VMEM)
    shapes = ((tok_rows, width),) + ((1, depth, cols),) * 3
    results = pl.pallas_call(
        functools.partial(layer, experts, copies, tps),
        out_shape=tuple(pltpu.VMEM(shape, BF16) for shape in shapes),
        in_specs=[anywhere] + [inside] * 3 + [anywhere] * 3,
        out_specs=(inside,) * 4,
        scratch_shapes=[
            pltpu.VMEM((tok_rows, width), BF16),
            pltpu.VMEM((shard, 1), F32),
            pltpu.VMEM((3, experts, shard, cols), F32),
            pltpu.VMEM((3, experts, shard, cols), BF16),
            pltpu.VMEM((n_rows, width), BF16),
            pltpu.VMEM((experts, experts, lanes), F32),
            pltpu.VMEM((experts, experts, lanes), F32),
            pltpu.VMEM((n_slots, width), BF16),
            pltpu.VMEM((half, tok_rows, 2 * CAP), BF16),
            pltpu.VMEM((n_slots, 128), F32),
            pltpu.VMEM((n_slots, cols), BF16),
            pltpu.VMEM((n_slots, width), BF16),
            pltpu.VMEM((tps - 1, n_slots, block), BF16),
            pltpu.VMEM((half, CAP, block), BF16),
            pltpu.VMEM((half, 2 * CAP, block), BF16),
            pltpu.VMEM((half * tok_rows, block), BF16),
            pltpu.VMEM(((half - 1) * tok_rows, block), BF16),
            dma((3, experts)),
            dma((3, experts, PARTS)),
            dma((3, experts, PARTS)),
            dma((3, experts, copies, PARTS)),
            dma((3, experts, copies, PARTS)),
            dma((experts,)),
            dma((experts,)),
            dma((experts,)),
            dma((experts,)),
            dma((experts, tps)),
            dma((experts, tps)),
            dma((experts, n_sub)),
            dma((tps - 1, n_w, n_sub)),
            dma((bits, n_w, n_sub)),
            dma((bits, n_w, n_sub)),
            dma((n_w, tps, n_sub)),
            dma((n_w, tps, n_sub)),
            dma,
        ],
        compiler_params=pltpu.CompilerParams(
            collective_id=0, has_side_effects=True, vmem_limit_bytes=KERNEL_VMEM
        ),
        name="layer",
    )(
        tokens,
        route_ids.T,
        route_logits.T,
        norm_gain[None, :],
        gate_weight,
        up_weight,
        down_weight,
    )
    return pl.pallas_call(
        store,
        out_shape=tuple(jax.ShapeDtypeStruct(shape, BF16) for shape in shapes),
        in_specs=[inside] * 4,
        out_specs=(anywhere,) * 4,
        scratch_shapes=[dma((4, STORES))],
        compiler_params=pltpu.CompilerParams(vmem_limit_bytes=1024 * 1024),
        name="store",
    )(*results)


def solution(mesh):
    return jax.shard_map(
        body,
        mesh=mesh,
        in_specs=(
            P("fs", None),
            P("fs", None),
            P("fs", None),
            P("fs"),
            P(None, "fs", "tp"),
            P(None, "fs", "tp"),
            P(None, "fs", "tp"),
        ),
        out_specs=(P("fs", None), P("fs", None, "tp"), P("fs", None, "tp"), P("fs", None, "tp")),
        check_vma=False,
    )
```
